32 devices in a mesh: kv: 8 (over z, core), tp: 4 (over y, x).
Axes of the slice: x: 2, y: 2, z: 4, core: 2. Of those that a mesh axis runs over, the one named last changes fastest.
Arguments:
- tokens: bfloat16 [128, 4096], P(None, 'kv'), may hold values from -40 to 40
- gain_first: float32 [4096], P('kv'), may hold values from 0.1 to 1.9
- gate_first: bfloat16 [4096, 11008], P('kv', 'tp'), may hold values from -0.09375 to 0.09375
- up_first: bfloat16 [4096, 11008], P('kv', 'tp'), may hold values from -0.09375 to 0.09375
- down_first: bfloat16 [11008, 4096], P('tp', 'kv'), may hold values from -0.0546875 to 0.0546875
- gain_mix: float32 [4096], P('kv'), may hold values from 0.1 to 1.9
- w_query: bfloat16 [4096, 2048], P('kv', 'tp'), may hold values from -0.09375 to 0.09375
- w_key: bfloat16 [4096, 2048], P('kv', 'tp'), may hold values from -0.09375 to 0.09375
- w_value: bfloat16 [4096, 2048], P('kv', 'tp'), may hold values from -0.09375 to 0.09375
- w_outgate: bfloat16 [4096, 2048], P('kv', 'tp'), may hold values from -0.09375 to 0.09375
- w_ingate: bfloat16 [4096, 16], P('kv'), may hold values from -0.046875 to 0.046875
- w_forget: bfloat16 [4096, 16], P('kv'), may hold values from -0.09375 to 0.09375
- forget_bias: float32 [16], P('tp'), may hold values from -1 to 4
- memory: float32 [128, 16, 128, 128], P('kv', 'tp'), may hold values from -0.6 to 0.6
- normalizer: float32 [128, 16, 128], P('kv', 'tp'), may hold values from -0.6 to 0.6
- stabilizer: float32 [128, 16], P('kv', 'tp'), may hold values from -3 to 0.5
- w_project: bfloat16 [2048, 4096], P('tp', 'kv'), may hold values from -0.75 to 0.75
- gain_second: float32 [4096], P('kv'), may hold values from 0.3 to 3
- gate_second: bfloat16 [4096, 11008], P('kv', 'tp'), may hold values from -0.09375 to 0.09375
- up_second: bfloat16 [4096, 11008], P('kv', 'tp'), may hold values from -0.09375 to 0.09375
- down_second: bfloat16 [11008, 4096], P('tp', 'kv'), may hold values from -0.0546875 to 0.0546875
Outputs:
- mixed_out: bfloat16 [128, 4096], P(None, 'kv')
- memory_new: float32 [128, 16, 128, 128], P('kv', 'tp')
- normalizer_new: float32 [128, 16, 128], P('kv', 'tp')
- stabilizer_new: float32 [128, 16], P('kv', 'tp')
The draws below stay inside these ranges and needn't reach their ends.
All inputs are finite; a program needn't handle non-finite values.
Results may differ from the reference program's by a relative error of at most 0.04.
Values may be sent and summed in bfloat16 or wider, within the bound.
A program may use at most 64 MiB of HBM per device.

```python
import math
import jax
import jax.numpy as jnp
from jax import lax

D = 4096
FF = 11008
H = 16
HD = 128
DM = 2048
B = 128
N_KV = 8


def draw_tokens(key, part):
    key_values, key_columns, key_scales = jax.random.split(key, 3)
    col_scales = jnp.exp(jnp.linspace(-1.0, 1.0, D)) * jax.random.uniform(key_columns, (D,), jnp.float32, 0.6, 1.4)
    values = jax.random.normal(key_values, (B, D), jnp.float32)
    row_scales = jnp.exp(jax.random.uniform(key_scales, (B, 1), jnp.float32, -1.1, 1.1))
    return jnp.clip(values * col_scales * row_scales, -40.0, 40.0).astype(jnp.bfloat16)


def block_levels(rng, dims, shards, low, top_value):
    level, own = 1.0, jax.random.fold_in(rng, 6)
    for axis_at, blocks in shards:
        draws = jnp.exp(jax.random.uniform(jax.random.fold_in(own, axis_at), (blocks,), jnp.float32, low / len(shards), top_value / len(shards)))
        level = level * jnp.repeat(draws, dims[axis_at] // blocks).reshape([-1 if axis == axis_at else 1 for axis in range(len(dims))])
    return level


def noise(stream_key, shape, spread, bound, cuts=(), kind=jnp.bfloat16):
    array = jax.random.normal(stream_key, shape, jnp.float32) * spread
    if len(cuts) > 0:
        array = block_levels(stream_key, shape, cuts, -0.22, 0.18) * array
    return jnp.clip(array, min=-bound, max=bound).astype(kind)


def setup_inputs(seed: int = 0) -> dict:
    key_list = jax.random.split(jax.random.key(seed), 22)
    tokens = draw_tokens(jax.random.fold_in(key_list[21], 71), 0)
    gain_first = jnp.clip(1.0 + 0.18 * jax.random.normal(key_list[1], (D,), jnp.float32), 0.1, 1.9)
    gate_first = noise(key_list[2], (D, FF), D ** -0.5, 0.09375, ((0, 8), (1, 4)))
    up_first = noise(key_list[3], (D, FF), D ** -0.5, 0.09375, ((0, 8), (1, 4)))
    down_first = noise(key_list[4], (FF, D), FF ** -0.5, 0.0546875, ((0, 4), (1, 8)))
    gain_mix = jnp.clip(1.0 + 0.18 * jax.random.normal(key_list[5], (D,), jnp.float32), 0.1, 1.9)
    w_query = noise(key_list[6], (D, DM), D ** -0.5, 0.09375, ((0, 8), (1, 4)))
    w_key = noise(key_list[7], (D, DM), D ** -0.5, 0.09375, ((0, 8), (1, 4)))
    w_value = noise(key_list[8], (D, DM), D ** -0.5, 0.09375, ((0, 8), (1, 4)))
    w_outgate = noise(key_list[9], (D, DM), D ** -0.5, 0.09375, ((0, 8), (1, 4)))
    w_ingate = noise(key_list[10], (D, H), (4 * D) ** -0.5, 0.046875, ((0, 8),))
    w_forget = noise(key_list[11], (D, H), D ** -0.5, 0.09375, ((0, 8),))
    forget_bias = jnp.clip(-1.0 + 5.0 * jax.random.uniform(key_list[12], (H,), jnp.float32) ** block_levels(key_list[12], (H,), ((0, 4),), -0.2, 0.2), -1.0, 4.0)
    memory = noise(key_list[13], (B, H, HD, HD), 0.1, 0.6, ((0, 8), (1, 4)), jnp.float32)
    normalizer = noise(key_list[14], (B, H, HD), 0.1, 0.6, ((0, 8), (1, 4)), jnp.float32)
    stabilizer = jnp.clip(-3.0 + 3.5 * jax.random.uniform(key_list[15], (B, H), jnp.float32) ** block_levels(key_list[15], (B, H), ((0, 8), (1, 4)), -0.2, 0.2), -3.0, 0.5)
    w_project = noise(key_list[16], (DM, D), (DM // 32) ** -0.5, 0.75, ((0, 4), (1, 8)))
    gain_second = jnp.clip(jnp.exp(math.log(3.0) - 2.3025851 * jax.random.uniform(key_list[17], (D,), jnp.float32) ** block_levels(key_list[17], (D,), ((0, 8),), -0.2, 0.2)), 0.3, 3.0)
    gate_second = noise(key_list[18], (D, FF), D ** -0.5, 0.09375, ((0, 8), (1, 4)))
    up_second = noise(key_list[19], (D, FF), D ** -0.5, 0.09375, ((0, 8), (1, 4)))
    down_second = noise(key_list[20], (FF, D), FF ** -0.5, 0.0546875, ((0, 4), (1, 8)))
    return dict(tokens=tokens, gain_first=gain_first, gate_first=gate_first, up_first=up_first, down_first=down_first, gain_mix=gain_mix, w_query=w_query, w_key=w_key, w_value=w_value, w_outgate=w_outgate, w_ingate=w_ingate, w_forget=w_forget, forget_bias=forget_bias, memory=memory, normalizer=normalizer, stabilizer=stabilizer, w_project=w_project, gain_second=gain_second, gate_second=gate_second, up_second=up_second, down_second=down_second)


EPSILON = 1e-06

def blockwise(scaled, weight):
    block_rows = weight.shape[0] // N_KV

    def add_block(index, running):
        block_start = index * block_rows
        partial_value = jnp.dot(lax.dynamic_slice_in_dim(scaled, block_start, block_rows, 1), lax.dynamic_slice_in_dim(weight, block_start, block_rows, 0), preferred_element_type=jnp.float32)
        rounded = lax.optimization_barrier(partial_value.astype(jnp.bfloat16))
        return running + rounded.astype(jnp.float32)
    return lax.fori_loop(0, N_KV, add_block, jnp.zeros((scaled.shape[0], weight.shape[1]), jnp.float32))

def row_scaling(widened):
    squared = lax.optimization_barrier(jnp.sum(widened * widened, axis=1, keepdims=True))
    return lax.rsqrt(squared / D + EPSILON)

def half_step(tokens, norm_gain, gate_weight, up_weight, down_weight):
    widened = tokens.astype(jnp.float32)
    row_scale = row_scaling(widened)
    scaled = (widened * norm_gain).astype(jnp.bfloat16)
    gate_values = row_scale * blockwise(scaled, gate_weight)
    up_values = row_scale * blockwise(scaled, up_weight)
    hidden = (jax.nn.silu(gate_values) * up_values).astype(jnp.bfloat16)
    down_values = jnp.dot(hidden, down_weight, preferred_element_type=jnp.float32)
    return (widened + 0.5 * down_values).astype(jnp.bfloat16)

def cell_update(query_bf, key_proj, value_proj, outgate, ingate, forget, memory, normalizer, stabilizer):
    seq_count, heads_here, head_size = normalizer.shape
    query_heads = query_bf.astype(jnp.float32).reshape(seq_count, heads_here, head_size)
    key_heads = key_proj.astype(jnp.float32).reshape(seq_count, heads_here, head_size) * head_size ** (-0.5)
    value_heads = value_proj.astype(jnp.float32).reshape(seq_count, heads_here, head_size)
    log_forget = jax.nn.log_sigmoid(forget)
    ceiling = jnp.maximum(log_forget + stabilizer, ingate)
    fresh_weight = jnp.exp(ingate - ceiling)
    carried = jnp.exp(log_forget + stabilizer - ceiling)
    own_score = lax.optimization_barrier(jnp.sum(query_heads * key_heads, axis=-1)) * fresh_weight
    recall = jnp.einsum('bhde,bhe->bhd', memory, query_heads, precision=lax.Precision.HIGHEST)
    numerator = own_score[..., None] * value_heads + carried[..., None] * recall
    denominator = own_score + carried * lax.optimization_barrier(jnp.sum(normalizer * query_heads, axis=-1))
    readout = numerator / jnp.maximum(jnp.abs(denominator), jnp.exp(-ceiling))[..., None]
    memory_new = carried[..., None, None] * memory + (fresh_weight[..., None] * value_heads)[..., :, None] * key_heads[..., None, :]
    normalizer_new = carried[..., None] * normalizer + fresh_weight[..., None] * key_heads
    gated_out = (jax.nn.sigmoid(outgate.astype(jnp.float32)) * readout.reshape(seq_count, -1)).astype(jnp.bfloat16)
    return (gated_out, memory_new, normalizer_new, ceiling)

def reference(tokens, gain_first, gate_first, up_first, down_first, gain_mix, w_query, w_key, w_value, w_outgate, w_ingate, w_forget, forget_bias, memory, normalizer, stabilizer, w_project, gain_second, gate_second, up_second, down_second):
    after_first = half_step(tokens, gain_first, gate_first, up_first, down_first)
    widened = after_first.astype(jnp.float32)
    row_scale = row_scaling(widened)
    scaled = (widened * gain_mix).astype(jnp.bfloat16)

    def project_heads(weight):
        return (row_scale * blockwise(scaled, weight)).astype(jnp.bfloat16)
    query_bf = project_heads(w_query)
    key_proj = project_heads(w_key)
    value_proj = project_heads(w_value)
    outgate = project_heads(w_outgate)
    ingate = row_scale * blockwise(scaled, w_ingate)
    forget = row_scale * blockwise(scaled, w_forget) + forget_bias
    gated_out, memory_new, normalizer_new, stabilizer_new = cell_update(query_bf, key_proj, value_proj, outgate, ingate, forget, memory, normalizer, stabilizer)
    after_mix = (widened + jnp.dot(gated_out, w_project, preferred_element_type=jnp.float32)).astype(jnp.bfloat16)
    mixed_out = half_step(after_mix, gain_second, gate_second, up_second, down_second)
    return (mixed_out, memory_new, normalizer_new, stabilizer_new)
```

```python
import functools
import math
from types import SimpleNamespace as NS

import jax
import jax.numpy as jnp
from jax import lax
from jax.experimental import pallas as pl
from jax.experimental.pallas import tpu as pltpu
from jax.sharding import PartitionSpec as P

EPSILON = 1e-06
LANES = 128
CHUNKS = 4
MESH = pl.DeviceIdType.MESH
BF = jnp.bfloat16
F32 = jnp.float32


def chunks_of(hidden):
    size = -(-hidden // (CHUNKS * 256)) * 256
    return [(at, min(size, hidden - at)) for at in range(0, hidden, size)]


def layer_kernel(n_kv, n_tp, unpack, *refs):
    arg, out, mem = unpack(refs)
    nz = n_kv // 2
    me = lax.axis_index("kv")
    z, c = me // 2, lax.rem(me, 2)
    tp = lax.axis_index("tp")
    partner = me + 1 - 2 * c
    rows, width = arg.tokens.shape
    d_model = width * n_kv
    rb = rows // n_kv
    rt = rows // n_tp
    head_size = arg.memory.shape[-1]
    heads = arg.memory.shape[1]

    loads = {}
    for i, (name, ref) in enumerate(mem.held.items()):
        loads[name] = pltpu.make_async_copy(getattr(arg, name), ref, mem.load_sem.at[i])
        loads[name].start()
    held = NS(**mem.held)
    load = NS(**loads)

    barrier = pltpu.get_barrier_semaphore()
    for d in range(1, n_kv):
        pl.semaphore_signal(barrier, inc=1, device_id={"kv": lax.rem(me + d, n_kv)}, device_id_type=MESH)
    for d in range(1, n_tp):
        pl.semaphore_signal(barrier, inc=1, device_id={"tp": lax.rem(tp + d, n_tp)}, device_id_type=MESH)

    def everyone_here():
        pl.semaphore_wait(barrier, n_kv + n_tp - 2)

    pending = []

    def remote(src, dst, send_sem, recv_sem, where):
        return pltpu.make_async_remote_copy(
            src_ref=src, dst_ref=dst, send_sem=send_sem, recv_sem=recv_sem, device_id=where, device_id_type=MESH)

    def send(*args):
        copy = remote(*args)
        copy.start()
        pending.append(copy)

    def arrived(dst, send_sem, recv_sem):
        remote(dst, dst, send_sem, recv_sem, {"kv": partner}).wait_recv()

    def flat(ref):
        a, b, w = ref.shape
        return ref[...].reshape(a * b, w)

    def norm_prepare(n, x, gain):
        wide = x.astype(F32)
        mem.scaled[...] = (wide * gain[...]).astype(BF)
        part = jnp.sum(wide * wide, axis=1, keepdims=True)
        n.sq_out[...] = jnp.broadcast_to(part, (rows, LANES)).reshape(n_kv, rb, LANES)

    def norm_send(n):
        for d in range(1, n_kv):
            peer = lax.rem(me + d, n_kv)
            send(n.sq_out.at[peer], n.sq_in.at[d], n.sq_s.at[d], n.sq_r.at[d], {"kv": peer})

    def norm_scale(n):
        total = n.sq_out[me]
        for d in range(1, n_kv):
            arrived(n.sq_in.at[d], n.sq_s.at[d], n.sq_r.at[d])
            total = total + n.sq_in[d]
        return lax.rsqrt(total / d_model + EPSILON)[:, :1]

    def rows_dot(weight):
        return lax.dot_general(
            mem.scaled[...], weight, (((1,), (1,)), ((), ())), preferred_element_type=F32).astype(BF)

    def keep(buf, g, val, place):
        for i in range(n_kv):
            buf[i % 2, i // 2, g, :, place] = val[i * rb:(i + 1) * rb]

    def product(weight, start, size, buf, g):
        step = 256
        full = size // step

        def tile(off, n, place):
            keep(buf, g, rows_dot(weight[pl.ds(off, n), :]), pl.ds(place, n))

        if full:
            @pl.loop(0, full)
            def _(t):
                tile(pl.multiple_of(start + t * step, 16), step, pl.multiple_of(t * step, step))
        if size > full * step:
            tile(start + full * step, size - full * step, full * step)

    def scatter_pair(s):
        for d in range(nz):
            chip = lax.rem(z + d + 1, nz)
            send(s.a.at[1 - c, chip], s.b.at[chip], s.s1.at[d], s.r1.at[d], {"kv": partner})

    def scatter_chips(s):
        for d in range(nz):
            chip = lax.rem(z + d + 1, nz)
            arrived(s.b.at[chip], s.s1.at[d], s.r1.at[d])
            if d < nz - 1:
                s.c[d] = (s.a[c, chip].astype(F32) + s.b[chip].astype(F32)).astype(BF)
                send(s.c.at[d], s.d.at[d], s.s2.at[d], s.r2.at[d], {"kv": chip * 2 + c})

    def scatter_sum(s):
        total = s.a[c, z].astype(F32) + s.b[z].astype(F32)
        for d in range(nz - 1):
            arrived(s.d.at[d], s.s2.at[d], s.r2.at[d])
            total = total + s.d[d].astype(F32)
        return total

    def gather_start(s):
        for d in range(nz - 1):
            chip = lax.rem(z + d + 1, nz)
            send(s.g.at[me], s.g.at[me], s.gs.at[d], s.gr.at[d], {"kv": chip * 2 + c})
        send(s.g.at[me], s.g.at[me], s.hs.at[nz - 1], s.hr.at[nz - 1], {"kv": partner})

    def gather_forward(s):
        for d in range(nz - 1):
            block = lax.rem(z - d - 1 + nz, nz) * 2 + c
            arrived(s.g.at[block], s.gs.at[d], s.gr.at[d])
            send(s.g.at[block], s.g.at[block], s.hs.at[d], s.hr.at[d], {"kv": partner})

    def gather_wait(s):
        for d in range(nz):
            block = lax.rem(z - d - 1 + nz, nz) * 2 + 1 - c
            arrived(s.g.at[block], s.hs.at[d], s.hr.at[d])

    def sum_tp(n, acc, residual, factor):
        mem.acc[...] = acc
        for j in range(n_tp):
            n.p[j] = acc[j * rt:(j + 1) * rt].astype(BF)
        for d in range(1, n_tp):
            peer = lax.rem(tp + d, n_tp)
            send(n.p.at[peer], n.q.at[d], n.ps.at[d], n.pr.at[d], {"tp": peer})
        total = mem.acc[pl.ds(pl.multiple_of(tp * rt, rt), rt)]
        for d in range(1, n_tp):
            arrived(n.q.at[d], n.ps.at[d], n.pr.at[d])
            total = total + n.q[d].astype(F32)
        n.o[tp] = (residual.astype(F32) + factor * total).astype(BF)
        for d in range(1, n_tp):
            peer = lax.rem(tp + d, n_tp)
            send(n.o.at[tp], n.o.at[tp], n.os.at[d], n.ur.at[d], {"tp": peer})
        for d in range(1, n_tp):
            source = lax.rem(tp - d + n_tp, n_tp)
            arrived(n.o.at[source], n.os.at[d], n.ur.at[d])

    def half_step(n, x, residual, gain, gate, up, down, load_gate, load_up, load_down, ready=None):
        norm_prepare(n, x, gain)
        if ready is None:
            norm_send(n)
        pieces = list(zip(chunks_of(gate.shape[0]), n.parts))
        load_gate.wait()
        for i, ((start, size), s) in enumerate(pieces):
            product(gate, start, size, s.a, 0)
            if i == 0:
                load_up.wait()
            product(up, start, size, s.a, 1)
            if i == 0 and ready is not None:
                ready()
                norm_send(n)
            scatter_pair(s)
            if i > 0:
                scatter_chips(pieces[i - 1][1])
        scatter_chips(pieces[-1][1])
        scale = norm_scale(n)
        for i, (_, s) in enumerate(pieces):
            total = scatter_sum(s)
            gate_values, up_values = scale * total[0], scale * total[1]
            s.g[me] = (gate_values / (1.0 + jnp.exp(-gate_values)) * up_values).astype(BF)
            gather_start(s)
        for _, s in pieces:
            gather_forward(s)
        load_down.wait()
        acc = jnp.zeros((rows, width), F32)
        for (start, size), s in pieces:
            gather_wait(s)
            acc = acc + jnp.dot(flat(s.g), down[start:start + size, :], preferred_element_type=F32)
        sum_tp(n, acc, residual(), 0.5)

    own_tp = pl.ds(pl.multiple_of(tp * rt, rt), rt)
    half_step(mem.first, arg.tokens[...], lambda: arg.tokens[own_tp], arg.gain_first, held.gate_first,
              held.up_first, held.down_first, load.gate_first, load.up_first, load.down_first,
              everyone_here)

    n = mem.mix
    norm_prepare(n, flat(mem.first.o), arg.gain_mix)
    norm_send(n)
    dm = arg.w_query.shape[1]
    n_heads = arg.w_ingate.shape[0]
    one, two = n.parts

    def wide_product(weight, s, at):
        val = jnp.dot(mem.scaled[...], weight[...], preferred_element_type=F32).astype(BF)
        keep(s.a, 0, val, slice(at, at + dm))

    load.w_query.wait()
    wide_product(held.w_query, one, 0)
    load.w_key.wait()
    wide_product(held.w_key, one, dm)
    gates = rows_dot(jnp.concatenate([arg.w_ingate[...], arg.w_forget[...]], axis=0))
    gates = jnp.concatenate([gates, jnp.zeros((rows, LANES - 2 * n_heads), BF)], axis=1)
    keep(one.a, 0, gates, slice(2 * dm, 2 * dm + LANES))
    scatter_pair(one)
    load.w_value.wait()
    wide_product(held.w_value, two, 0)
    load.w_outgate.wait()
    wide_product(held.w_outgate, two, dm)
    scatter_pair(two)
    scatter_chips(one)
    scatter_chips(two)
    scale = norm_scale(n)
    total = scale * scatter_sum(one)[0]
    total_two = scale * scatter_sum(two)[0]

    gates = total[:, 2 * dm:]
    lane = lax.broadcasted_iota(jnp.int32, (rb, LANES), 1)
    diagonal = lax.broadcasted_iota(jnp.int32, (rb, rb), 0) == lax.broadcasted_iota(jnp.int32, (rb, rb), 1)
    load.memory.wait()
    state = held.memory
    parts = []
    for h in range(heads):
        low, high = h * head_size, (h + 1) * head_size
        q, k, v, gate_out = (
            val.astype(BF).astype(F32)
            for val in (total[:, low:high], total[:, dm + low:dm + high],
                        total_two[:, low:high], total_two[:, dm + low:dm + high]))
        k = k * head_size ** (-0.5)
        ingate = jnp.sum(jnp.where(lane == tp * heads + h, gates, 0.0), axis=1, keepdims=True)
        forget = jnp.sum(jnp.where(lane == n_heads + tp * heads + h, gates, 0.0), axis=1, keepdims=True)
        forget = forget + arg.forget_bias[h]
        log_forget = jnp.minimum(forget, 0.0) - jnp.log1p(jnp.exp(-jnp.abs(forget)))
        stabilizer = jnp.sum(jnp.where(diagonal, arg.stabilizer[h:h + 1, :], 0.0), axis=1, keepdims=True)
        kept = log_forget + stabilizer
        ceiling = jnp.maximum(kept, ingate)
        fresh = jnp.exp(ingate - ceiling)
        carried = jnp.exp(kept - ceiling)
        out.stabilizer_new[h:h + 1, :] = jnp.sum(jnp.where(diagonal, ceiling, 0.0), axis=0, keepdims=True)
        norm = arg.normalizer[:, h, :]
        out.normalizer_new[:, h, :] = carried * norm + fresh * k
        own = jnp.sum(q * k, axis=1, keepdims=True) * fresh
        den = own + carried * jnp.sum(norm * q, axis=1, keepdims=True)
        den = jnp.maximum(jnp.abs(den), jnp.exp(-ceiling))
        mem.row_q[h] = q
        mem.row_k[h] = fresh * k
        mem.row_c[h] = jnp.broadcast_to(carried, (rb, head_size))
        pad = jnp.zeros((LANES - rb, head_size), F32)
        mem.col_v[h] = jnp.concatenate([v, pad], axis=0).T
        mem.col_r[h] = jnp.zeros((head_size, LANES), F32)
        parts.append((own, v, carried, den, gate_out))

    lane2 = lax.broadcasted_iota(jnp.int32, (head_size, LANES), 1)

    @pl.loop(0, rb)
    def _(b):
        for h in range(heads):
            recall = jnp.sum(state[b, h] * mem.row_q[h, pl.ds(b, 1), :], axis=1, keepdims=True)
            mem.col_r[h] = jnp.where(lane2 == b, recall, mem.col_r[h])

    for h in range(heads):
        own, v, carried, den, gate_out = parts[h]
        recall = mem.col_r[h].T[:rb]
        readout = (own * v + carried * recall) / den
        n.parts[0].g[me, :, h * head_size:(h + 1) * head_size] = (
            readout / (1.0 + jnp.exp(-gate_out))).astype(BF)
    gather_start(one)

    @pl.loop(0, rb)
    def _(b):
        for h in range(heads):
            v_col = jnp.sum(jnp.where(lane2 == b, mem.col_v[h], 0.0), axis=1, keepdims=True)
            state[b, h] = (mem.row_c[h, pl.ds(b, 1), :] * state[b, h]
                           + v_col * mem.row_k[h, pl.ds(b, 1), :])

    store = pltpu.make_async_copy(state, out.memory_new, mem.load_sem.at[len(mem.held)])
    store.start()
    gather_forward(one)
    load.w_project.wait()
    gather_wait(one)
    sum_tp(n, jnp.dot(flat(one.g), held.w_project[...], preferred_element_type=F32), mem.first.o[tp], 1.0)

    half_step(mem.second, flat(n.o), lambda: n.o[tp], arg.gain_second, held.gate_second,
              held.up_second, held.down_second, load.gate_second, load.up_second, load.down_second)
    out.mixed_out[...] = flat(mem.second.o)
    store.wait()
    for copy in pending:
        copy.wait_send()


def results_kernel(mixed, normalizer, stabilizer, memory, mixed_out, normalizer_out, stabilizer_out, memory_out,
                   held, in_sem, out_sem):
    count = in_sem.shape[0]
    size = held.shape[0] // count

    def piece(i):
        return pl.ds(i * size, size)

    ins = [pltpu.make_async_copy(memory.at[piece(i)], held.at[piece(i)], in_sem.at[i]) for i in range(count)]
    outs = [pltpu.make_async_copy(held.at[piece(i)], memory_out.at[piece(i)], out_sem.at[i]) for i in range(count)]
    for copy in ins:
        copy.start()
    mixed_out[...] = mixed[...]
    normalizer_out[...] = normalizer[...]
    stabilizer_out[...] = stabilizer[...]
    for into, out in zip(ins, outs):
        into.wait()
        out.start()
    for copy in outs:
        copy.wait()


def on_device(
    n_kv, n_tp, tokens, gain_first, gate_first, up_first, down_first, gain_mix, w_query, w_key, w_value,
    w_outgate, w_ingate, w_forget, forget_bias, memory, normalizer, stabilizer, w_project, gain_second,
    gate_second, up_second, down_second,
):
    rows, width = tokens.shape
    hidden = gate_first.shape[1]
    dm = w_query.shape[1]
    nz, rb, rt = n_kv // 2, rows // n_kv, rows // n_tp
    heads, head_size = memory.shape[1], memory.shape[3]
    dma = pltpu.SemaphoreType.DMA

    in_vmem = dict(
        tokens=tokens, gain_first=gain_first.reshape(1, -1), gain_mix=gain_mix.reshape(1, -1),
        gain_second=gain_second.reshape(1, -1), w_ingate=w_ingate.T, w_forget=w_forget.T,
        normalizer=normalizer, stabilizer=stabilizer.T)
    in_smem = dict(forget_bias=forget_bias)
    streamed = dict(
        gate_first=gate_first.T, up_first=up_first.T, down_first=down_first, w_query=w_query, w_key=w_key,
        w_value=w_value, w_outgate=w_outgate, memory=memory, w_project=w_project, gate_second=gate_second.T,
        up_second=up_second.T, down_second=down_second)
    operands = {**in_vmem, **in_smem, **streamed}
    results = dict(
        mixed_out=jax.ShapeDtypeStruct(tokens.shape, BF),
        memory_new=jax.ShapeDtypeStruct(memory.shape, F32),
        normalizer_new=jax.ShapeDtypeStruct(normalizer.shape, F32),
        stabilizer_new=jax.ShapeDtypeStruct(stabilizer.shape[::-1], F32))

    def exchange(g, cols, gathered):
        bufs = dict(
            a=pltpu.VMEM((2, nz, g, rb, cols), BF), b=pltpu.VMEM((nz, g, rb, cols), BF),
            c=pltpu.VMEM((nz, g, rb, cols), BF), d=pltpu.VMEM((nz, g, rb, cols), BF),
            s1=dma((nz,)), r1=dma((nz,)), s2=dma((nz,)), r2=dma((nz,)))
        if gathered:
            bufs.update(
                g=pltpu.VMEM((n_kv, rb, gathered), BF), gs=dma((nz,)), gr=dma((nz,)), hs=dma((nz,)), hr=dma((nz,)))
        return bufs

    def phase(parts):
        return dict(
            parts=parts,
            sq_out=pltpu.VMEM((n_kv, rb, LANES), F32), sq_in=pltpu.VMEM((n_kv, rb, LANES), F32),
            sq_s=dma((n_kv,)), sq_r=dma((n_kv,)),
            p=pltpu.VMEM((n_tp, rt, width), BF), q=pltpu.VMEM((n_tp, rt, width), BF),
            o=pltpu.VMEM((n_tp, rt, width), BF),
            ps=dma((n_tp,)), pr=dma((n_tp,)), os=dma((n_tp,)), ur=dma((n_tp,)))

    tree = dict(
        held={name: pltpu.VMEM(a.shape, a.dtype) for name, a in streamed.items()},
        load_sem=dma((len(streamed) + 1,)),
        scaled=pltpu.VMEM((rows, width), BF),
        acc=pltpu.VMEM((rows, width), F32),
        first=phase([exchange(2, size, size) for _, size in chunks_of(hidden)]),
        mix=phase([exchange(1, 2 * dm + LANES, dm), exchange(1, 2 * dm, 0)]),
        second=phase([exchange(2, size, size) for _, size in chunks_of(hidden)]),
        row_q=pltpu.VMEM((heads, rb, head_size), F32),
        row_k=pltpu.VMEM((heads, rb, head_size), F32),
        row_c=pltpu.VMEM((heads, rb, head_size), F32),
        col_v=pltpu.VMEM((heads, head_size, LANES), F32),
        col_r=pltpu.VMEM((heads, head_size, LANES), F32))

    shapes = []

    def number(node):
        if isinstance(node, dict):
            return {key: number(value) for key, value in node.items()}
        if isinstance(node, list):
            return [number(value) for value in node]
        shapes.append(node)
        return len(shapes) - 1

    numbered = number(tree)

    def unpack(refs):
        n_in, n_out = len(operands), len(results)
        scratch = refs[n_in + n_out:]

        def fill(node):
            if isinstance(node, dict):
                return NS(**{key: fill(value) for key, value in node.items()})
            if isinstance(node, list):
                return [fill(value) for value in node]
            return scratch[node]

        mem = fill(numbered)
        mem.held = {name: scratch[i] for name, i in numbered["held"].items()}
        return NS(**dict(zip(operands, refs))), NS(**dict(zip(results, refs[n_in:]))), mem

    vm = pl.BlockSpec(memory_space=pltpu.VMEM)
    hbm = pl.BlockSpec(memory_space=pl.ANY)
    mixed_out, memory_new, normalizer_new, stabilizer_new = pl.pallas_call(
        functools.partial(layer_kernel, n_kv, n_tp, unpack),
        out_shape=list(results.values()),
        in_specs=[vm] * len(in_vmem) + [pl.BlockSpec(memory_space=pltpu.SMEM)] + [hbm] * len(streamed),
        out_specs=[vm, hbm, vm, vm],
        scratch_shapes=shapes,
        compiler_params=pltpu.CompilerParams(
            collective_id=0, has_side_effects=True, vmem_limit_bytes=60 * 2**20),
    )(*operands.values())
    count = math.gcd(rb, 8)
    mixed_out, normalizer_new, stabilizer_new, memory_new = pl.pallas_call(
        results_kernel,
        out_shape=[results[name] for name in ("mixed_out", "normalizer_new", "stabilizer_new", "memory_new")],
        in_specs=[vm, vm, vm, hbm],
        out_specs=[vm, vm, vm, hbm],
        scratch_shapes=[pltpu.VMEM(memory.shape, F32), dma((count,)), dma((count,))],
    )(mixed_out, normalizer_new, stabilizer_new, memory_new)
    return mixed_out, memory_new, normalizer_new, stabilizer_new.T


def solution(mesh):
    kv, tp, both = P("kv"), P("tp"), P("kv", "tp")
    width, back = P(None, "kv"), P("tp", "kv")
    return jax.shard_map(
        functools.partial(on_device, mesh.shape["kv"], mesh.shape["tp"]),
        mesh=mesh,
        in_specs=(width, kv, both, both, back, kv, both, both, both, both, kv, kv, tp, both, both, both,
                  back, kv, both, both, back),
        out_specs=(width, both, both, both),
        check_vma=False,
    )
```

```python
import functools
import math
from types import SimpleNamespace as NS

import jax
import jax.numpy as jnp
from jax import lax
from jax.experimental import pallas as pl
from jax.experimental.pallas import tpu as pltpu
from jax.sharding import PartitionSpec as P

EPSILON = 1e-06
LANES = 128
CHUNKS = 4
MESH = pl.DeviceIdType.MESH
BF = jnp.bfloat16
F32 = jnp.float32


def chunks_of(hidden):
    size = -(-hidden // (CHUNKS * 256)) * 256
    return [(at, min(size, hidden - at)) for at in range(0, hidden, size)]


def layer_kernel(n_kv, n_tp, unpack, *refs):
    arg, out, mem = unpack(refs)
    nz = n_kv // 2
    me = lax.axis_index("kv")
    z, c = me // 2, lax.rem(me, 2)
    tp = lax.axis_index("tp")
    partner = me + 1 - 2 * c
    rows, width = arg.tokens.shape
    d_model = width * n_kv
    rb = rows // n_kv
    rt = rows // n_tp
    head_size = arg.memory.shape[-1]
    heads = arg.memory.shape[1]

    loads = {}
    for i, (name, ref) in enumerate(mem.held.items()):
        loads[name] = pltpu.make_async_copy(getattr(arg, name), ref, mem.load_sem.at[i])
        loads[name].start()
    held = NS(**mem.held)
    load = NS(**loads)

    barrier = pltpu.get_barrier_semaphore()
    for d in range(1, n_kv):
        pl.semaphore_signal(barrier, inc=1, device_id={"kv": lax.rem(me + d, n_kv)}, device_id_type=MESH)
    for d in range(1, n_tp):
        pl.semaphore_signal(barrier, inc=1, device_id={"tp": lax.rem(tp + d, n_tp)}, device_id_type=MESH)

    def everyone_here():
        pl.semaphore_wait(barrier, n_kv + n_tp - 2)

    pending = []

    def remote(src, dst, send_sem, recv_sem, where):
        return pltpu.make_async_remote_copy(
            src_ref=src, dst_ref=dst, send_sem=send_sem, recv_sem=recv_sem, device_id=where, device_id_type=MESH)

    def send(*args):
        remote(*args).start()
        pending.append(args)

    def arrived(dst, send_sem, recv_sem):
        remote(dst, dst, send_sem, recv_sem, {"kv": partner}).wait_recv()

    def flat(ref):
        a, b, w = ref.shape
        return ref[...].reshape(a * b, w)

    def rows_of(ref):
        return lambda own=None: flat(ref) if own is None else ref[tp]

    def norm_prepare(n, x, gain):
        wide = x.astype(F32)
        mem.scaled[...] = (wide * gain[...]).astype(BF)
        part = jnp.sum(wide * wide, axis=1, keepdims=True)
        n.sq_out[...] = jnp.broadcast_to(part, (rows, LANES)).reshape(n_kv, rb, LANES)

    def norm_send(n):
        for d in range(1, n_kv):
            peer = lax.rem(me + d, n_kv)
            send(n.sq_out.at[peer], n.sq_in.at[d], n.sq_s.at[d], n.sq_r.at[d], {"kv": peer})

    def norm_scale(n):
        total = n.sq_out[me]
        for d in range(1, n_kv):
            arrived(n.sq_in.at[d], n.sq_s.at[d], n.sq_r.at[d])
            total = total + n.sq_in[d]
        return lax.rsqrt(total / d_model + EPSILON)[:, :1]

    def rows_dot(weight):
        return lax.dot_general(
            mem.scaled[...], weight, (((1,), (1,)), ((), ())), preferred_element_type=F32).astype(BF)

    def keep(buf, g, val, place):
        for i in range(n_kv):
            buf[i % 2, i // 2, g, :, place] = val[i * rb:(i + 1) * rb]

    def product(weight, start, size, buf, g):
        step = 256
        full = size // step

        def tile(off, n, place):
            keep(buf, g, rows_dot(weight[pl.ds(off, n), :]), pl.ds(place, n))

        if full:
            @pl.loop(0, full)
            def _(t):
                tile(pl.multiple_of(start + t * step, 16), step, pl.multiple_of(t * step, step))
        if size > full * step:
            tile(start + full * step, size - full * step, full * step)

    def scatter_pair(s):
        for d in range(nz):
            chip = lax.rem(z + d + 1, nz)
            send(s.a.at[1 - c, chip], s.b.at[chip], s.s1.at[d], s.r1.at[d], {"kv": partner})

    def scatter_chips(s):
        for d in range(nz):
            chip = lax.rem(z + d + 1, nz)
            arrived(s.b.at[chip], s.s1.at[d], s.r1.at[d])
            if d < nz - 1:
                s.c[d] = (s.a[c, chip].astype(F32) + s.b[chip].astype(F32)).astype(BF)
                send(s.c.at[d], s.d.at[d], s.s2.at[d], s.r2.at[d], {"kv": chip * 2 + c})

    def scatter_sum(s):
        total = s.a[c, z].astype(F32) + s.b[z].astype(F32)
        for d in range(nz - 1):
            arrived(s.d.at[d], s.s2.at[d], s.r2.at[d])
            total = total + s.d[d].astype(F32)
        return total

    def gather_start(s):
        for d in range(nz - 1):
            chip = lax.rem(z + d + 1, nz)
            send(s.g.at[me], s.g.at[me], s.gs.at[d], s.gr.at[d], {"kv": chip * 2 + c})
        send(s.g.at[me], s.g.at[me], s.hs.at[nz - 1], s.hr.at[nz - 1], {"kv": partner})

    def gather_forward(s):
        for d in range(nz - 1):
            block = lax.rem(z - d - 1 + nz, nz) * 2 + c
            arrived(s.g.at[block], s.gs.at[d], s.gr.at[d])
            send(s.g.at[block], s.g.at[block], s.hs.at[d], s.hr.at[d], {"kv": partner})

    def gather_wait(s):
        for d in range(nz):
            block = lax.rem(z - d - 1 + nz, nz) * 2 + 1 - c
            arrived(s.g.at[block], s.hs.at[d], s.hr.at[d])

    line = nz == 4
    at_end = (z == 0) | (z == nz - 1)
    mate = z + 1 - 2 * lax.rem(z, 2)
    far_middle = jnp.where(z < 2, 2, 1)
    far_end = jnp.where(z < 2, 3, 0)
    far = (far_middle, far_end)

    def chip_sum(s, chip):
        return s.a[c, chip].astype(F32) + s.b[chip].astype(F32)

    def line_send_out(s):
        for d in range(nz):
            chip = lax.rem(z + d + 1, nz)
            arrived(s.b.at[chip], s.s1.at[d], s.r1.at[d])

        @pl.when(at_end)
        def _():
            for j in range(2):
                s.c[j] = chip_sum(s, far[j]).astype(BF)
                remote(s.c.at[j], s.e.at[j], s.s2.at[j], s.re.at[j], {"kv": mate * 2 + c}).start()

        @pl.when(jnp.logical_not(at_end))
        def _():
            line_send_mate(s)

    def line_send_mate(s):
        s.c[2] = chip_sum(s, mate).astype(BF)
        remote(s.c.at[2], s.d.at[0], s.s2.at[2], s.r2.at[0], {"kv": mate * 2 + c}).start()

    def line_pass(s):
        @pl.when(at_end)
        def _():
            line_send_mate(s)

        @pl.when(jnp.logical_not(at_end))
        def _():
            for j in range(2):
                arrived(s.e.at[j], s.s2.at[j], s.re.at[j])
                s.c[j] = (chip_sum(s, far[j]) + s.e[j].astype(F32)).astype(BF)
                remote(s.c.at[j], s.d.at[1], s.s2.at[j], s.r2.at[1], {"kv": far[j] * 2 + c}).start()

        for j in range(3):
            pending.append((s.c.at[j], s.d.at[0], s.s2.at[j], s.r2.at[0], {"kv": mate * 2 + c}))

    def line_sum(s):
        total = chip_sum(s, z)
        for j in range(2):
            arrived(s.d.at[j], s.s2.at[j], s.r2.at[j])
            total = total + s.d[j].astype(F32)
        return total

    def line_gather_start(s):
        send(s.g.at[me], s.g.at[me], s.gs.at[0], s.gr.at[0], {"kv": mate * 2 + c})
        send(s.g.at[me], s.g.at[me], s.gs.at[1], s.gr.at[jnp.where(at_end, 2, 1)], {"kv": far_middle * 2 + c})
        send(s.g.at[me], s.g.at[me], s.hs.at[nz - 1], s.hr.at[nz - 1], {"kv": partner})

    def line_gather_forward(s):
        for j, chip in enumerate((mate, far_middle, far_end)):
            block = chip * 2 + c
            arrived(s.g.at[block], s.gs.at[j], s.gr.at[j])
            if j > 0:
                @pl.when(jnp.logical_not(at_end))
                def _():
                    remote(s.g.at[block], s.g.at[block], s.gs.at[j + 1], s.gr.at[j], {"kv": mate * 2 + c}).start()
            send(s.g.at[block], s.g.at[block], s.hs.at[j], s.hr.at[j], {"kv": partner})

    def line_gather_wait(s):
        for j, chip in enumerate((mate, far_middle, far_end, z)):
            arrived(s.g.at[chip * 2 + 1 - c], s.hs.at[j], s.hr.at[j])

    def line_gather_sent(s):
        @pl.when(jnp.logical_not(at_end))
        def _():
            for j in range(1, 3):
                block = far[j - 1] * 2 + c
                remote(s.g.at[block], s.g.at[block], s.gs.at[j + 1], s.gr.at[j], {"kv": mate * 2 + c}).wait_send()

    def sum_tp(n, acc, residual, factor):
        if n_tp == 4:
            sum_tp_exchange(n, acc, residual(), factor)
        else:
            sum_tp_scatter(n, acc, residual(own_tp), factor)

    def sum_tp_exchange(n, acc, residual, factor):
        half = width // 2
        sub = rows // 2
        one, two = tp + 1 - 2 * lax.rem(tp, 2), lax.rem(tp + 2, 4)
        order = [(k, r) for r in range(2) for k in range(2)]

        def part(val, k, r):
            return val[r * sub:(r + 1) * sub, k * half:(k + 1) * half]

        def swap(step, k, r):
            i = (step * 2 + k) * 2 + r
            return n.p.at[i], n.q.at[i], n.ps.at[i], n.pr.at[i], {"tp": one if k == step else two}

        for k, r in order:
            n.p[k * 2 + r] = part(acc, k, r).astype(BF)
            send(*swap(0, k, r))
        for k, r in order:
            i = k * 2 + r
            arrived(n.q.at[i], n.ps.at[i], n.pr.at[i])
            n.p[4 + i] = (n.p[i].astype(F32) + n.q[i].astype(F32)).astype(BF)
            send(*swap(1, k, r))
        for k, r in order:
            i = 4 + k * 2 + r
            arrived(n.q.at[i], n.ps.at[i], n.pr.at[i])
            total = n.p[i].astype(F32) + n.q[i].astype(F32)
            val = (part(residual, k, r).astype(F32) + factor * total).astype(BF)
            n.o[r * 2:(r + 1) * 2, :, k * half:(k + 1) * half] = val.reshape(2, rt, half)

    def sum_tp_scatter(n, acc, residual, factor):
        mem.acc[...] = acc
        for j in range(n_tp):
            n.p[j] = acc[j * rt:(j + 1) * rt].astype(BF)
        for d in range(1, n_tp):
            peer = lax.rem(tp + d, n_tp)
            send(n.p.at[peer], n.q.at[d], n.ps.at[d], n.pr.at[d], {"tp": peer})
        total = mem.acc[pl.ds(pl.multiple_of(tp * rt, rt), rt)]
        for d in range(1, n_tp):
            arrived(n.q.at[d], n.ps.at[d], n.pr.at[d])
            total = total + n.q[d].astype(F32)
        n.o[tp] = (residual.astype(F32) + factor * total).astype(BF)
        for d in range(1, n_tp):
            peer = lax.rem(tp + d, n_tp)
            send(n.o.at[tp], n.o.at[tp], n.os.at[d], n.ur.at[d], {"tp": peer})
        for d in range(1, n_tp):
            source = lax.rem(tp - d + n_tp, n_tp)
            arrived(n.o.at[source], n.os.at[d], n.ur.at[d])

    def half_step(n, x, residual, gain, gate, up, down, load_gate, load_up, load_down, ready=None):
        norm_prepare(n, x, gain)
        if ready is None:
            norm_send(n)
        pieces = list(zip(chunks_of(gate.shape[0]), n.parts))
        load_gate.wait()
        for i, ((start, size), s) in enumerate(pieces):
            product(gate, start, size, s.a, 0)
            if i == 0:
                load_up.wait()
            product(up, start, size, s.a, 1)
            if i == 0 and ready is not None:
                ready()
                norm_send(n)
            scatter_pair(s)
            if i > 0:
                (line_send_out if line else scatter_chips)(pieces[i - 1][1])
        (line_send_out if line else scatter_chips)(pieces[-1][1])
        scale = norm_scale(n)
        if line:
            for _, s in pieces:
                line_pass(s)
        for i, (_, s) in enumerate(pieces):
            total = (line_sum if line else scatter_sum)(s)
            gate_values, up_values = scale * total[0], scale * total[1]
            s.g[me] = (gate_values / (1.0 + jnp.exp(-gate_values)) * up_values).astype(BF)
            (line_gather_start if line else gather_start)(s)
        for _, s in pieces:
            (line_gather_forward if line else gather_forward)(s)
        load_down.wait()
        acc = jnp.zeros((rows, width), F32)
        for (start, size), s in pieces:
            (line_gather_wait if line else gather_wait)(s)
            acc = acc + jnp.dot(flat(s.g), down[start:start + size, :], preferred_element_type=F32)
        sum_tp(n, acc, residual, 0.5)
        if line:
            for _, s in pieces:
                line_gather_sent(s)

    own_tp = pl.ds(pl.multiple_of(tp * rt, rt), rt)
    half_step(mem.first, arg.tokens[...], lambda own=slice(None): arg.tokens[own], arg.gain_first, held.gate_first,
              held.up_first, held.down_first, load.gate_first, load.up_first, load.down_first,
              everyone_here)

    n = mem.mix
    norm_prepare(n, flat(mem.first.o), arg.gain_mix)
    norm_send(n)
    dm = arg.w_query.shape[1]
    n_heads = arg.w_ingate.shape[0]
    one, two = n.parts

    def wide_product(weight, s, at):
        val = jnp.dot(mem.scaled[...], weight[...], preferred_element_type=F32).astype(BF)
        keep(s.a, 0, val, slice(at, at + dm))

    load.w_query.wait()
    wide_product(held.w_query, one, 0)
    load.w_key.wait()
    wide_product(held.w_key, one, dm)
    gates = rows_dot(jnp.concatenate([arg.w_ingate[...], arg.w_forget[...]], axis=0))
    gates = jnp.concatenate([gates, jnp.zeros((rows, LANES - 2 * n_heads), BF)], axis=1)
    keep(one.a, 0, gates, slice(2 * dm, 2 * dm + LANES))
    scatter_pair(one)
    load.w_value.wait()
    wide_product(held.w_value, two, 0)
    load.w_outgate.wait()
    wide_product(held.w_outgate, two, dm)
    scatter_pair(two)
    scatter_chips(one)
    scatter_chips(two)
    scale = norm_scale(n)
    total = scale * scatter_sum(one)[0]
    total_two = scale * scatter_sum(two)[0]

    gates = total[:, 2 * dm:]
    lane = lax.broadcasted_iota(jnp.int32, (rb, LANES), 1)
    diagonal = lax.broadcasted_iota(jnp.int32, (rb, rb), 0) == lax.broadcasted_iota(jnp.int32, (rb, rb), 1)
    load.memory.wait()
    state = held.memory
    parts = []
    for h in range(heads):
        low, high = h * head_size, (h + 1) * head_size
        q, k, v, gate_out = (
            val.astype(BF).astype(F32)
            for val in (total[:, low:high], total[:, dm + low:dm + high],
                        total_two[:, low:high], total_two[:, dm + low:dm + high]))
        k = k * head_size ** (-0.5)
        ingate = jnp.sum(jnp.where(lane == tp * heads + h, gates, 0.0), axis=1, keepdims=True)
        forget = jnp.sum(jnp.where(lane == n_heads + tp * heads + h, gates, 0.0), axis=1, keepdims=True)
        forget = forget + arg.forget_bias[h]
        log_forget = jnp.minimum(forget, 0.0) - jnp.log1p(jnp.exp(-jnp.abs(forget)))
        stabilizer = jnp.sum(jnp.where(diagonal, arg.stabilizer[h:h + 1, :], 0.0), axis=1, keepdims=True)
        kept = log_forget + stabilizer
        ceiling = jnp.maximum(kept, ingate)
        fresh = jnp.exp(ingate - ceiling)
        carried = jnp.exp(kept - ceiling)
        out.stabilizer_new[h:h + 1, :] = jnp.sum(jnp.where(diagonal, ceiling, 0.0), axis=0, keepdims=True)
        norm = arg.normalizer[:, h, :]
        out.normalizer_new[:, h, :] = carried * norm + fresh * k
        own = jnp.sum(q * k, axis=1, keepdims=True) * fresh
        den = own + carried * jnp.sum(norm * q, axis=1, keepdims=True)
        den = jnp.maximum(jnp.abs(den), jnp.exp(-ceiling))
        mem.row_q[h] = q
        mem.row_k[h] = fresh * k
        mem.row_c[h] = jnp.broadcast_to(carried, (rb, head_size))
        pad = jnp.zeros((LANES - rb, head_size), F32)
        mem.col_v[h] = jnp.concatenate([v, pad], axis=0).T
        mem.col_r[h] = jnp.zeros((head_size, LANES), F32)
        parts.append((own, v, carried, den, gate_out))

    lane2 = lax.broadcasted_iota(jnp.int32, (head_size, LANES), 1)

    @pl.loop(0, rb)
    def _(b):
        for h in range(heads):
            recall = jnp.sum(state[b, h] * mem.row_q[h, pl.ds(b, 1), :], axis=1, keepdims=True)
            mem.col_r[h] = jnp.where(lane2 == b, recall, mem.col_r[h])

    for h in range(heads):
        own, v, carried, den, gate_out = parts[h]
        recall = mem.col_r[h].T[:rb]
        readout = (own * v + carried * recall) / den
        n.parts[0].g[me, :, h * head_size:(h + 1) * head_size] = (
            readout / (1.0 + jnp.exp(-gate_out))).astype(BF)
    gather_start(one)

    @pl.loop(0, rb)
    def _(b):
        for h in range(heads):
            v_col = jnp.sum(jnp.where(lane2 == b, mem.col_v[h], 0.0), axis=1, keepdims=True)
            state[b, h] = (mem.row_c[h, pl.ds(b, 1), :] * state[b, h]
                           + v_col * mem.row_k[h, pl.ds(b, 1), :])

    store = pltpu.make_async_copy(state, out.memory_new, mem.load_sem.at[len(mem.held)])
    store.start()
    gather_forward(one)
    load.w_project.wait()
    gather_wait(one)
    sum_tp(n, jnp.dot(flat(one.g), held.w_project[...], preferred_element_type=F32), rows_of(mem.first.o), 1.0)

    half_step(mem.second, flat(n.o), rows_of(n.o), arg.gain_second, held.gate_second,
              held.up_second, held.down_second, load.gate_second, load.up_second, load.down_second)
    out.mixed_out[...] = flat(mem.second.o)
    store.wait()
    for args in pending:
        remote(*args).wait_send()


def results_kernel(count, n, *refs):
    sources, targets, held, (in_sem, out_sem) = refs[:n], refs[n:2 * n], refs[2 * n:3 * n], refs[3 * n:]
    pieces = []
    for source, target, ref in zip(sources, targets, held):
        cuts = count if source is sources[0] else 1
        size = ref.shape[0] // cuts
        for i in range(cuts):
            at = pl.ds(i * size, size)
            sems = len(pieces)
            pieces.append((
                pltpu.make_async_copy(source.at[at], ref.at[at], in_sem.at[sems]),
                pltpu.make_async_copy(ref.at[at], target.at[at], out_sem.at[sems])))
    for into, _ in pieces:
        into.start()
    for into, out in pieces:
        into.wait()
        out.start()
    for _, out in pieces:
        out.wait()


def on_device(
    n_kv, n_tp, tokens, gain_first, gate_first, up_first, down_first, gain_mix, w_query, w_key, w_value,
    w_outgate, w_ingate, w_forget, forget_bias, memory, normalizer, stabilizer, w_project, gain_second,
    gate_second, up_second, down_second,
):
    rows, width = tokens.shape
    hidden = gate_first.shape[1]
    dm = w_query.shape[1]
    nz, rb, rt = n_kv // 2, rows // n_kv, rows // n_tp
    heads, head_size = memory.shape[1], memory.shape[3]
    dma = pltpu.SemaphoreType.DMA

    in_vmem = dict(
        tokens=tokens, gain_first=gain_first.reshape(1, -1), gain_mix=gain_mix.reshape(1, -1),
        gain_second=gain_second.reshape(1, -1), w_ingate=w_ingate.T, w_forget=w_forget.T,
        normalizer=normalizer, stabilizer=stabilizer.T)
    in_smem = dict(forget_bias=forget_bias)
    streamed = dict(
        gate_first=gate_first.T, up_first=up_first.T, down_first=down_first, w_query=w_query, w_key=w_key,
        w_value=w_value, w_outgate=w_outgate, memory=memory, w_project=w_project, gate_second=gate_second.T,
        up_second=up_second.T, down_second=down_second)
    operands = {**in_vmem, **in_smem, **streamed}
    results = dict(
        mixed_out=jax.ShapeDtypeStruct(tokens.shape, BF),
        memory_new=jax.ShapeDtypeStruct(memory.shape, F32),
        normalizer_new=jax.ShapeDtypeStruct(normalizer.shape, F32),
        stabilizer_new=jax.ShapeDtypeStruct(stabilizer.shape[::-1], F32))

    def exchange(g, cols, gathered):
        bufs = dict(
            a=pltpu.VMEM((2, nz, g, rb, cols), BF), b=pltpu.VMEM((nz, g, rb, cols), BF),
            c=pltpu.VMEM((nz, g, rb, cols), BF), d=pltpu.VMEM((nz, g, rb, cols), BF),
            s1=dma((nz,)), r1=dma((nz,)), s2=dma((nz,)), r2=dma((nz,)))
        if g == 2 and nz == 4:
            bufs.update(e=pltpu.VMEM((2, g, rb, cols), BF), re=dma((2,)))
        if gathered:
            bufs.update(
                g=pltpu.VMEM((n_kv, rb, gathered), BF), gs=dma((nz,)), gr=dma((nz,)), hs=dma((nz,)), hr=dma((nz,)))
        return bufs

    swap = (8, rows // 2, width // 2) if n_tp == 4 else (n_tp, rt, width)

    def phase(parts):
        return dict(
            parts=parts,
            sq_out=pltpu.VMEM((n_kv, rb, LANES), F32), sq_in=pltpu.VMEM((n_kv, rb, LANES), F32),
            sq_s=dma((n_kv,)), sq_r=dma((n_kv,)),
            p=pltpu.VMEM(swap, BF), q=pltpu.VMEM(swap, BF), o=pltpu.VMEM((n_tp, rt, width), BF),
            ps=dma(swap[:1]), pr=dma(swap[:1]), os=dma((n_tp,)), ur=dma((n_tp,)))

    tree = dict(
        held={name: pltpu.VMEM(a.shape, a.dtype) for name, a in streamed.items()},
        load_sem=dma((len(streamed) + 1,)),
        scaled=pltpu.VMEM((rows, width), BF),
        acc=pltpu.VMEM((rows, width), F32),
        first=phase([exchange(2, size, size) for _, size in chunks_of(hidden)]),
        mix=phase([exchange(1, 2 * dm + LANES, dm), exchange(1, 2 * dm, 0)]),
        second=phase([exchange(2, size, size) for _, size in chunks_of(hidden)]),
        row_q=pltpu.VMEM((heads, rb, head_size), F32),
        row_k=pltpu.VMEM((heads, rb, head_size), F32),
        row_c=pltpu.VMEM((heads, rb, head_size), F32),
        col_v=pltpu.VMEM((heads, head_size, LANES), F32),
        col_r=pltpu.VMEM((heads, head_size, LANES), F32))

    shapes = []

    def number(node):
        if isinstance(node, dict):
            return {key: number(value) for key, value in node.items()}
        if isinstance(node, list):
            return [number(value) for value in node]
        shapes.append(node)
        return len(shapes) - 1

    numbered = number(tree)

    def unpack(refs):
        n_in, n_out = len(operands), len(results)
        scratch = refs[n_in + n_out:]

        def fill(node):
            if isinstance(node, dict):
                return NS(**{key: fill(value) for key, value in node.items()})
            if isinstance(node, list):
                return [fill(value) for value in node]
            return scratch[node]

        mem = fill(numbered)
        mem.held = {name: scratch[i] for name, i in numbered["held"].items()}
        return NS(**dict(zip(operands, refs))), NS(**dict(zip(results, refs[n_in:]))), mem

    vm = pl.BlockSpec(memory_space=pltpu.VMEM)
    hbm = pl.BlockSpec(memory_space=pl.ANY)
    mixed_out, memory_new, normalizer_new, stabilizer_new = pl.pallas_call(
        functools.partial(layer_kernel, n_kv, n_tp, unpack),
        out_shape=list(results.values()),
        in_specs=[vm] * len(in_vmem) + [pl.BlockSpec(memory_space=pltpu.SMEM)] + [hbm] * len(streamed),
        out_specs=[vm, hbm, vm, vm],
        scratch_shapes=shapes,
        compiler_params=pltpu.CompilerParams(
            collective_id=0, has_side_effects=True, vmem_limit_bytes=60 * 2**20),
    )(*operands.values())
    count = math.gcd(rb, 8)
    passed = [memory_new, mixed_out, normalizer_new, stabilizer_new]
    memory_new, mixed_out, normalizer_new, stabilizer_new = pl.pallas_call(
        functools.partial(results_kernel, count, len(passed)),
        out_shape=[jax.ShapeDtypeStruct(a.shape, a.dtype) for a in passed],
        in_specs=[hbm] * len(passed),
        out_specs=[hbm] * len(passed),
        scratch_shapes=[pltpu.VMEM(a.shape, a.dtype) for a in passed]
        + [dma((count + len(passed) - 1,)), dma((count + len(passed) - 1,))],
    )(*passed)
    return mixed_out, memory_new, normalizer_new, stabilizer_new.T


def solution(mesh):
    kv, tp, both = P("kv"), P("tp"), P("kv", "tp")
    width, back = P(None, "kv"), P("tp", "kv")
    return jax.shard_map(
        functools.partial(on_device, mesh.shape["kv"], mesh.shape["tp"]),
        mesh=mesh,
        in_specs=(width, kv, both, both, back, kv, both, both, both, both, kv, kv, tp, both, both, both,
                  back, kv, both, both, back),
        out_specs=(width, both, both, both),
        check_vma=False,
    )
```

```python
import functools
import math
from types import SimpleNamespace as NS

import jax
import jax.numpy as jnp
from jax import lax
from jax.experimental import pallas as pl
from jax.experimental.pallas import tpu as pltpu
from jax.sharding import PartitionSpec as P

EPSILON = 1e-06
LANES = 128
TILE = 256
PACE = (3, 3, 3, 2)
DIRECT = 1
LAG = 9
READY = 0
BLOCKS = 4
MESH = pl.DeviceIdType.MESH
BF = jnp.bfloat16
F32 = jnp.float32


def chunks_of(hidden):
    tiles = -(-hidden // TILE)
    total, passed, cuts = sum(PACE), 0, [0]
    for share in PACE:
        passed += share
        cut = min(hidden, (tiles * passed + total // 2) // total * TILE)
        if cut > cuts[-1]:
            cuts.append(cut)
    return [(low, high - low) for low, high in zip(cuts, cuts[1:])]


def layer_kernel(n_kv, n_tp, unpack, *refs):
    arg, out, mem = unpack(refs)
    nz = n_kv // 2
    me = lax.axis_index("kv")
    z, c = me // 2, lax.rem(me, 2)
    tp = lax.axis_index("tp")
    partner = me + 1 - 2 * c
    rows, width = arg.tokens.shape
    d_model = width * n_kv
    rb = rows // n_kv
    rt = rows // n_tp
    head_size = arg.memory.shape[-1]
    heads = arg.memory.shape[1]

    pieces_of = chunks_of(arg.gate_first.shape[0])
    relayed = max(len(pieces_of) - DIRECT, 0)
    held = NS(**mem.held)
    loads = {}

    def begin(name, cuts=None):
        source, target = getattr(arg, name), mem.held[name]
        for cut in cuts or [None]:
            at = slice(None) if cut is None else pl.ds(*cut)
            sem = mem.load_sem.at[sum(len(made) for made in loads.values())]
            copy = pltpu.make_async_copy(source.at[at], target.at[at], sem)
            copy.start()
            loads.setdefault(name, []).append(copy)

    def loaded(name, i=None):
        for copy in loads[name] if i is None else [loads[name][i]]:
            copy.wait()

    begin("tokens")
    begin("gain_first")
    for cut in pieces_of:
        begin("gate_first", [cut])
        begin("up_first", [cut])
    for name in mem.held:
        if name not in loads:
            begin(name)

    barrier = pltpu.get_barrier_semaphore()
    for d in range(1, n_kv):
        pl.semaphore_signal(barrier, inc=1, device_id={"kv": lax.rem(me + d, n_kv)}, device_id_type=MESH)
    for d in range(1, n_tp):
        pl.semaphore_signal(barrier, inc=1, device_id={"tp": lax.rem(tp + d, n_tp)}, device_id_type=MESH)

    def everyone_here():
        pl.semaphore_wait(barrier, n_kv + n_tp - 2)

    pending = []

    def remote(src, dst, send_sem, recv_sem, where):
        return pltpu.make_async_remote_copy(
            src_ref=src, dst_ref=dst, send_sem=send_sem, recv_sem=recv_sem, device_id=where, device_id_type=MESH)

    def send(*args):
        remote(*args).start()
        pending.append(args)

    def arrived(dst, send_sem, recv_sem):
        remote(dst, dst, send_sem, recv_sem, {"kv": partner}).wait_recv()

    def flat(ref):
        a, b, w = ref.shape
        return ref[...].reshape(a * b, w)

    def rows_of(ref):
        return lambda own=None: flat(ref) if own is None else ref[tp]

    def norm_prepare(n, x, gain):
        wide = x.astype(F32)
        mem.scaled[...] = (wide * gain[...]).astype(BF)
        part = jnp.sum(wide * wide, axis=1, keepdims=True)
        n.sq_out[...] = jnp.broadcast_to(part, (rows, LANES)).reshape(n_kv, rb, LANES)

    def norm_send(n):
        for d in range(1, n_kv):
            peer = lax.rem(me + d, n_kv)
            send(n.sq_out.at[peer], n.sq_in.at[d], n.sq_s.at[d], n.sq_r.at[d], {"kv": peer})

    def norm_scale(n):
        total = n.sq_out[me]
        for d in range(1, n_kv):
            arrived(n.sq_in.at[d], n.sq_s.at[d], n.sq_r.at[d])
            total = total + n.sq_in[d]
        return lax.rsqrt(total / d_model + EPSILON)[:, :1]

    def rows_dot(weight):
        return lax.dot_general(
            mem.scaled[...], weight, (((1,), (1,)), ((), ())), preferred_element_type=F32).astype(BF)

    def keep(buf, g, val, place):
        for i in range(n_kv):
            buf[i % 2, i // 2, g, :, place] = val[i * rb:(i + 1) * rb]

    def product(weight, start, size, buf, g):
        step = TILE
        full = size // step

        def tile(off, n, place):
            keep(buf, g, rows_dot(weight[pl.ds(off, n), :]), pl.ds(place, n))

        if full:
            @pl.loop(0, full)
            def _(t):
                tile(pl.multiple_of(start + t * step, 16), step, pl.multiple_of(t * step, step))
        if size > full * step:
            tile(start + full * step, size - full * step, full * step)

    def scatter_pair(s):
        for d in range(nz):
            chip = lax.rem(z + d + 1, nz)
            send(s.a.at[1 - c, chip], s.b.at[chip], s.s1.at[d], s.r1.at[d], {"kv": partner})

    def scatter_chips(s):
        for d in range(nz):
            chip = lax.rem(z + d + 1, nz)
            arrived(s.b.at[chip], s.s1.at[d], s.r1.at[d])
            if d < nz - 1:
                s.c[d] = (s.a[c, chip].astype(F32) + s.b[chip].astype(F32)).astype(BF)
                send(s.c.at[d], s.d.at[d], s.s2.at[d], s.r2.at[d], {"kv": chip * 2 + c})

    def scatter_sum(s):
        total = s.a[c, z].astype(F32) + s.b[z].astype(F32)
        for d in range(nz - 1):
            arrived(s.d.at[d], s.s2.at[d], s.r2.at[d])
            total = total + s.d[d].astype(F32)
        return total

    def gather_start(s):
        for d in range(nz - 1):
            chip = lax.rem(z + d + 1, nz)
            send(s.g.at[me], s.g.at[me], s.gs.at[d], s.gr.at[d], {"kv": chip * 2 + c})
        send(s.g.at[me], s.g.at[me], s.hs.at[nz - 1], s.hr.at[nz - 1], {"kv": partner})

    def gather_forward(s):
        for d in range(nz - 1):
            block = lax.rem(z - d - 1 + nz, nz) * 2 + c
            arrived(s.g.at[block], s.gs.at[d], s.gr.at[d])
            send(s.g.at[block], s.g.at[block], s.hs.at[d], s.hr.at[d], {"kv": partner})

    def gather_wait(s):
        for d in range(nz):
            block = lax.rem(z - d - 1 + nz, nz) * 2 + 1 - c
            arrived(s.g.at[block], s.hs.at[d], s.hr.at[d])

    line = nz == 4
    at_end = (z == 0) | (z == nz - 1)
    mate = z + 1 - 2 * lax.rem(z, 2)
    far_middle = jnp.where(z < 2, 2, 1)
    far_end = jnp.where(z < 2, 3, 0)
    far = (far_middle, far_end)

    def chip_sum(s, chip):
        return s.a[c, chip].astype(F32) + s.b[chip].astype(F32)

    def line_send_out(s):
        for d in range(nz):
            chip = lax.rem(z + d + 1, nz)
            arrived(s.b.at[chip], s.s1.at[d], s.r1.at[d])

        @pl.when(at_end)
        def _():
            for j in (1, 0):
                s.c[j] = chip_sum(s, far[j]).astype(BF)
                remote(s.c.at[j], s.e.at[j], s.s2.at[j], s.re.at[j], {"kv": mate * 2 + c}).start()

        @pl.when(jnp.logical_not(at_end))
        def _():
            line_send_mate(s)

    def line_send_mate(s):
        s.c[2] = chip_sum(s, mate).astype(BF)
        remote(s.c.at[2], s.d.at[0], s.s2.at[2], s.r2.at[0], {"kv": mate * 2 + c}).start()

    def line_follow(s):
        @pl.when(at_end)
        def _():
            line_send_mate(s)

    def line_pass(s):
        @pl.when(jnp.logical_not(at_end))
        def _():
            for j in (1, 0):
                arrived(s.e.at[j], s.s2.at[j], s.re.at[j])
                s.c[j] = (chip_sum(s, far[j]) + s.e[j].astype(F32)).astype(BF)
                remote(s.c.at[j], s.d.at[1], s.s2.at[j], s.r2.at[1], {"kv": far[j] * 2 + c}).start()

        for j in range(3):
            pending.append((s.c.at[j], s.d.at[0], s.s2.at[j], s.r2.at[0], {"kv": mate * 2 + c}))

    def line_sum(s):
        total = chip_sum(s, z)
        for j in range(2):
            arrived(s.d.at[j], s.s2.at[j], s.r2.at[j])
            total = total + s.d[j].astype(F32)
        return total

    mine = jnp.where(at_end, 2, 1)

    def line_gather_start(s, direct):
        send(s.g.at[me], s.g.at[me], s.gs.at[0], s.gr.at[0], {"kv": mate * 2 + c})
        for j in range(2 if direct else 1):
            send(s.g.at[me], s.g.at[me], s.gs.at[1 + j], s.gr.at[mine], {"kv": far[j] * 2 + c})
        send(s.g.at[me], s.g.at[me], s.hs.at[nz - 1], s.hr.at[nz - 1], {"kv": partner})

    def line_gather_forward(s, direct):
        for j, chip in enumerate((mate, far_middle, far_end)):
            block = chip * 2 + c
            arrived(s.g.at[block], s.gs.at[j], s.gr.at[j])
            if j > 0 and not direct:
                @pl.when(jnp.logical_not(at_end))
                def _():
                    remote(s.g.at[block], s.g.at[block], s.gs.at[j + 1], s.gr.at[j], {"kv": mate * 2 + c}).start()
            send(s.g.at[block], s.g.at[block], s.hs.at[j], s.hr.at[j], {"kv": partner})

    def line_gather_wait(s):
        for j, chip in enumerate((mate, far_middle, far_end, z)):
            arrived(s.g.at[chip * 2 + 1 - c], s.hs.at[j], s.hr.at[j])

    def line_gather_sent(s):
        @pl.when(jnp.logical_not(at_end))
        def _():
            for j in range(1, 3):
                block = far[j - 1] * 2 + c
                remote(s.g.at[block], s.g.at[block], s.gs.at[j + 1], s.gr.at[j], {"kv": mate * 2 + c}).wait_send()

    def sum_tp(n, acc, residual, factor):
        if n_tp == BLOCKS:
            sum_tp_exchange(n, acc, residual(), factor)
        else:
            sum_tp_scatter(n, acc, residual(own_tp), factor)

    def sum_tp_exchange(n, acc, residual, factor):
        half = width // 2
        sub = rows // BLOCKS
        one, two = tp + 1 - 2 * lax.rem(tp, 2), lax.rem(tp + 2, 4)
        order = [(k, r) for r in range(BLOCKS) for k in range(2)]

        def part(val, k, r):
            return val[r * sub:(r + 1) * sub, k * half:(k + 1) * half]

        def swap(step, k, r):
            i = (step * 2 + k) * BLOCKS + r
            return n.p.at[i], n.q.at[i], n.ps.at[i], n.pr.at[i], {"tp": one if k == step else two}

        for k, r in order:
            n.p[k * BLOCKS + r] = part(acc, k, r).astype(BF)
            send(*swap(0, k, r))
        for k, r in order:
            i = k * BLOCKS + r
            arrived(n.q.at[i], n.ps.at[i], n.pr.at[i])
            n.p[2 * BLOCKS + i] = (n.p[i].astype(F32) + n.q[i].astype(F32)).astype(BF)
            send(*swap(1, k, r))
        for k, r in order:
            i = (2 + k) * BLOCKS + r
            arrived(n.q.at[i], n.ps.at[i], n.pr.at[i])
            total = n.p[i].astype(F32) + n.q[i].astype(F32)
            val = (part(residual, k, r).astype(F32) + factor * total).astype(BF)
            n.o[r, :, k * half:(k + 1) * half] = val

    def sum_tp_scatter(n, acc, residual, factor):
        mem.acc[...] = acc
        for j in range(n_tp):
            n.p[j] = acc[j * rt:(j + 1) * rt].astype(BF)
        for d in range(1, n_tp):
            peer = lax.rem(tp + d, n_tp)
            send(n.p.at[peer], n.q.at[d], n.ps.at[d], n.pr.at[d], {"tp": peer})
        total = mem.acc[pl.ds(pl.multiple_of(tp * rt, rt), rt)]
        for d in range(1, n_tp):
            arrived(n.q.at[d], n.ps.at[d], n.pr.at[d])
            total = total + n.q[d].astype(F32)
        n.o[tp] = (residual.astype(F32) + factor * total).astype(BF)
        for d in range(1, n_tp):
            peer = lax.rem(tp + d, n_tp)
            send(n.o.at[tp], n.o.at[tp], n.os.at[d], n.ur.at[d], {"tp": peer})
        for d in range(1, n_tp):
            source = lax.rem(tp - d + n_tp, n_tp)
            arrived(n.o.at[source], n.os.at[d], n.ur.at[d])

    def send_out(pieces, i):
        if not line:
            scatter_chips(pieces[i][1])
            return
        line_send_out(pieces[i][1])
        if i >= LAG:
            line_follow(pieces[i - LAG][1])

    def half_step(label, n, x, residual, ready=None):
        gate, up, down = (mem.held[name + label] for name in ("gate_", "up_", "down_"))
        norm_prepare(n, x, mem.held["gain_" + label])
        if ready is None:
            norm_send(n)
        pieces = list(zip(pieces_of, n.parts))
        by_piece = len(loads["gate_" + label]) > 1
        held_back = min(READY, len(pieces) - 1)
        for i, ((start, size), s) in enumerate(pieces):
            if by_piece or i == 0:
                loaded("gate_" + label, i)
            product(gate, start, size, s.a, 0)
            if by_piece or i == 0:
                loaded("up_" + label, i)
            product(up, start, size, s.a, 1)
            if ready is not None and i < held_back:
                continue
            if ready is not None and i == held_back:
                ready()
                norm_send(n)
                for _, earlier in pieces[:i]:
                    scatter_pair(earlier)
            scatter_pair(s)
            for j in range(0 if i == held_back and ready is not None else max(i - 1, 0), i):
                send_out(pieces, j)
        send_out(pieces, len(pieces) - 1)
        scale = norm_scale(n)
        if line:
            for _, s in pieces[max(len(pieces) - LAG, 0):]:
                line_follow(s)
            for _, s in pieces:
                line_pass(s)
        for i, (_, s) in enumerate(pieces):
            total = (line_sum if line else scatter_sum)(s)
            gate_values, up_values = scale * total[0], scale * total[1]
            s.g[me] = (gate_values / (1.0 + jnp.exp(-gate_values)) * up_values).astype(BF)
            if line:
                line_gather_start(s, i >= relayed)
            else:
                gather_start(s)
        for i, (_, s) in enumerate(pieces):
            if line:
                line_gather_forward(s, i >= relayed)
            else:
                gather_forward(s)
        loaded("down_" + label)
        acc = jnp.zeros((rows, width), F32)
        for (start, size), s in pieces:
            (line_gather_wait if line else gather_wait)(s)
            acc = acc + jnp.dot(flat(s.g), down[start:start + size, :], preferred_element_type=F32)
        sum_tp(n, acc, residual, 0.5)
        if line:
            for _, s in pieces[:relayed]:
                line_gather_sent(s)

    own_tp = pl.ds(pl.multiple_of(tp * rt, rt), rt)
    loaded("tokens")
    loaded("gain_first")
    half_step("first", mem.first, held.tokens[...], lambda own=slice(None): held.tokens[own], everyone_here)
    for name in ("gain_mix", "w_ingate", "w_forget", "normalizer", "stabilizer", "gain_second"):
        loaded(name)

    n = mem.mix
    norm_prepare(n, flat(mem.first.o), held.gain_mix)
    norm_send(n)
    dm = held.w_query.shape[1]
    n_heads = held.w_ingate.shape[0]
    one, two = n.parts

    def wide_product(weight, s, at):
        val = jnp.dot(mem.scaled[...], weight[...], preferred_element_type=F32).astype(BF)
        keep(s.a, 0, val, slice(at, at + dm))

    loaded("w_query")
    wide_product(held.w_query, one, 0)
    loaded("w_key")
    wide_product(held.w_key, one, dm)
    gates = rows_dot(jnp.concatenate([held.w_ingate[...], held.w_forget[...]], axis=0))
    gates = jnp.concatenate([gates, jnp.zeros((rows, LANES - 2 * n_heads), BF)], axis=1)
    keep(one.a, 0, gates, slice(2 * dm, 2 * dm + LANES))
    scatter_pair(one)
    loaded("w_value")
    wide_product(held.w_value, two, 0)
    loaded("w_outgate")
    wide_product(held.w_outgate, two, dm)
    scatter_pair(two)
    scatter_chips(one)
    scatter_chips(two)
    scale = norm_scale(n)
    total = scale * scatter_sum(one)[0]
    total_two = scale * scatter_sum(two)[0]

    gates = total[:, 2 * dm:]
    lane = lax.broadcasted_iota(jnp.int32, (rb, LANES), 1)
    diagonal = lax.broadcasted_iota(jnp.int32, (rb, rb), 0) == lax.broadcasted_iota(jnp.int32, (rb, rb), 1)
    loaded("memory")
    state = held.memory
    parts = []
    for h in range(heads):
        low, high = h * head_size, (h + 1) * head_size
        q, k, v, gate_out = (
            val.astype(BF).astype(F32)
            for val in (total[:, low:high], total[:, dm + low:dm + high],
                        total_two[:, low:high], total_two[:, dm + low:dm + high]))
        k = k * head_size ** (-0.5)
        ingate = jnp.sum(jnp.where(lane == tp * heads + h, gates, 0.0), axis=1, keepdims=True)
        forget = jnp.sum(jnp.where(lane == n_heads + tp * heads + h, gates, 0.0), axis=1, keepdims=True)
        forget = forget + arg.forget_bias[h]
        log_forget = jnp.minimum(forget, 0.0) - jnp.log1p(jnp.exp(-jnp.abs(forget)))
        stabilizer = jnp.sum(jnp.where(diagonal, held.stabilizer[h:h + 1, :], 0.0), axis=1, keepdims=True)
        kept = log_forget + stabilizer
        ceiling = jnp.maximum(kept, ingate)
        fresh = jnp.exp(ingate - ceiling)
        carried = jnp.exp(kept - ceiling)
        out.stabilizer_new[h:h + 1, :] = jnp.sum(jnp.where(diagonal, ceiling, 0.0), axis=0, keepdims=True)
        norm = held.normalizer[:, h, :]
        out.normalizer_new[:, h, :] = carried * norm + fresh * k
        own = jnp.sum(q * k, axis=1, keepdims=True) * fresh
        den = own + carried * jnp.sum(norm * q, axis=1, keepdims=True)
        den = jnp.maximum(jnp.abs(den), jnp.exp(-ceiling))
        mem.row_q[h] = q
        mem.row_k[h] = fresh * k
        mem.row_c[h] = jnp.broadcast_to(carried, (rb, head_size))
        pad = jnp.zeros((LANES - rb, head_size), F32)
        mem.col_v[h] = jnp.concatenate([v, pad], axis=0).T
        parts.append((own, v, carried, den, gate_out))

    lane2 = lax.broadcasted_iota(jnp.int32, (head_size, LANES), 1)
    row = lax.broadcasted_iota(jnp.int32, (rb, head_size), 0)
    queries = [mem.row_q[h].astype(BF) for h in range(heads)]
    together = math.gcd(rb, 4)

    def recall_step(step, found):
        for at in range(together):
            b = step * together + at
            found = tuple(
                jnp.where(row == b, lax.dot_general(
                    queries[h], state[b, h].astype(BF), (((1,), (1,)), ((), ())), preferred_element_type=F32), found[h])
                for h in range(heads))
        return found

    nothing = jnp.zeros((rb, head_size), F32)
    recalls = lax.fori_loop(0, rb // together, recall_step, (nothing,) * heads)

    for h in range(heads):
        own, v, carried, den, gate_out = parts[h]
        recall = recalls[h]
        readout = (own * v + carried * recall) / den
        n.parts[0].g[me, :, h * head_size:(h + 1) * head_size] = (
            readout / (1.0 + jnp.exp(-gate_out))).astype(BF)
    gather_start(one)

    @pl.loop(0, rb)
    def _(b):
        for h in range(heads):
            v_col = jnp.sum(jnp.where(lane2 == b, mem.col_v[h], 0.0), axis=1, keepdims=True)
            state[b, h] = (mem.row_c[h, pl.ds(b, 1), :] * state[b, h]
                           + v_col * mem.row_k[h, pl.ds(b, 1), :])

    store = pltpu.make_async_copy(state, out.memory_new, mem.load_sem.at[sum(len(made) for made in loads.values())])
    store.start()
    gather_forward(one)
    loaded("w_project")
    gather_wait(one)
    sum_tp(n, jnp.dot(flat(one.g), held.w_project[...], preferred_element_type=F32), rows_of(mem.first.o), 1.0)

    half_step("second", mem.second, flat(n.o), rows_of(n.o))
    out.mixed_out[...] = flat(mem.second.o)
    store.wait()
    for args in pending:
        remote(*args).wait_send()


def results_kernel(count, n, *refs):
    sources, targets, held, (in_sem, out_sem) = refs[:n], refs[n:2 * n], refs[2 * n:3 * n], refs[3 * n:]
    pieces = []
    for source, target, ref in zip(sources, targets, held):
        cuts = count if source is sources[0] else 1
        size = ref.shape[0] // cuts
        for i in range(cuts):
            at = pl.ds(i * size, size)
            sems = len(pieces)
            pieces.append((
                pltpu.make_async_copy(source.at[at], ref.at[at], in_sem.at[sems]),
                pltpu.make_async_copy(ref.at[at], target.at[at], out_sem.at[sems])))
    for into, _ in pieces:
        into.start()
    for into, out in pieces:
        into.wait()
        out.start()
    for _, out in pieces:
        out.wait()


def on_device(
    n_kv, n_tp, tokens, gain_first, gate_first, up_first, down_first, gain_mix, w_query, w_key, w_value,
    w_outgate, w_ingate, w_forget, forget_bias, memory, normalizer, stabilizer, w_project, gain_second,
    gate_second, up_second, down_second,
):
    rows, width = tokens.shape
    hidden = gate_first.shape[1]
    dm = w_query.shape[1]
    nz, rb, rt = n_kv // 2, rows // n_kv, rows // n_tp
    heads, head_size = memory.shape[1], memory.shape[3]
    dma = pltpu.SemaphoreType.DMA

    in_smem = dict(forget_bias=forget_bias)
    streamed = dict(
        tokens=tokens, gain_first=gain_first.reshape(1, -1), gate_first=gate_first.T, up_first=up_first.T,
        down_first=down_first, gain_mix=gain_mix.reshape(1, -1), w_ingate=w_ingate.T, w_forget=w_forget.T,
        w_query=w_query, w_key=w_key, w_value=w_value, w_outgate=w_outgate, normalizer=normalizer,
        stabilizer=stabilizer.T, memory=memory, w_project=w_project, gain_second=gain_second.reshape(1, -1),
        gate_second=gate_second.T, up_second=up_second.T, down_second=down_second)
    operands = {**in_smem, **streamed}
    results = dict(
        mixed_out=jax.ShapeDtypeStruct(tokens.shape, BF),
        memory_new=jax.ShapeDtypeStruct(memory.shape, F32),
        normalizer_new=jax.ShapeDtypeStruct(normalizer.shape, F32),
        stabilizer_new=jax.ShapeDtypeStruct(stabilizer.shape[::-1], F32))

    def exchange(g, cols, gathered):
        bufs = dict(
            a=pltpu.VMEM((2, nz, g, rb, cols), BF), b=pltpu.VMEM((nz, g, rb, cols), BF),
            c=pltpu.VMEM((nz, g, rb, cols), BF), d=pltpu.VMEM((nz, g, rb, cols), BF),
            s1=dma((nz,)), r1=dma((nz,)), s2=dma((nz,)), r2=dma((nz,)))
        if g == 2 and nz == 4:
            bufs.update(e=pltpu.VMEM((2, g, rb, cols), BF), re=dma((2,)))
        if gathered:
            bufs.update(
                g=pltpu.VMEM((n_kv, rb, gathered), BF), gs=dma((nz,)), gr=dma((nz,)), hs=dma((nz,)), hr=dma((nz,)))
        return bufs

    swap = (4 * BLOCKS, rows // BLOCKS, width // 2) if n_tp == BLOCKS else (n_tp, rt, width)

    def phase(parts):
        return dict(
            parts=parts,
            sq_out=pltpu.VMEM((n_kv, rb, LANES), F32), sq_in=pltpu.VMEM((n_kv, rb, LANES), F32),
            sq_s=dma((n_kv,)), sq_r=dma((n_kv,)),
            p=pltpu.VMEM(swap, BF), q=pltpu.VMEM(swap, BF), o=pltpu.VMEM((n_tp, rt, width), BF),
            ps=dma(swap[:1]), pr=dma(swap[:1]), os=dma((n_tp,)), ur=dma((n_tp,)))

    tree = dict(
        held={name: pltpu.VMEM(a.shape, a.dtype) for name, a in streamed.items()},
        load_sem=dma((len(streamed) + 2 * len(chunks_of(hidden)),)),
        scaled=pltpu.VMEM((rows, width), BF),
        acc=pltpu.VMEM((rows, width), F32),
        first=phase([exchange(2, size, size) for _, size in chunks_of(hidden)]),
        mix=phase([exchange(1, 2 * dm + LANES, dm), exchange(1, 2 * dm, 0)]),
        second=phase([exchange(2, size, size) for _, size in chunks_of(hidden)]),
        row_q=pltpu.VMEM((heads, rb, head_size), F32),
        row_k=pltpu.VMEM((heads, rb, head_size), F32),
        row_c=pltpu.VMEM((heads, rb, head_size), F32),
        col_v=pltpu.VMEM((heads, head_size, LANES), F32))

    shapes = []

    def number(node):
        if isinstance(node, dict):
            return {key: number(value) for key, value in node.items()}
        if isinstance(node, list):
            return [number(value) for value in node]
        shapes.append(node)
        return len(shapes) - 1

    numbered = number(tree)

    def unpack(refs):
        n_in, n_out = len(operands), len(results)
        scratch = refs[n_in + n_out:]

        def fill(node):
            if isinstance(node, dict):
                return NS(**{key: fill(value) for key, value in node.items()})
            if isinstance(node, list):
                return [fill(value) for value in node]
            return scratch[node]

        mem = fill(numbered)
        mem.held = {name: scratch[i] for name, i in numbered["held"].items()}
        return NS(**dict(zip(operands, refs))), NS(**dict(zip(results, refs[n_in:]))), mem

    vm = pl.BlockSpec(memory_space=pltpu.VMEM)
    hbm = pl.BlockSpec(memory_space=pl.ANY)
    mixed_out, memory_new, normalizer_new, stabilizer_new = pl.pallas_call(
        functools.partial(layer_kernel, n_kv, n_tp, unpack),
        out_shape=list(results.values()),
        in_specs=[pl.BlockSpec(memory_space=pltpu.SMEM)] + [hbm] * len(streamed),
        out_specs=[vm, hbm, vm, vm],
        scratch_shapes=shapes,
        compiler_params=pltpu.CompilerParams(
            collective_id=0, has_side_effects=True, vmem_limit_bytes=60 * 2**20),
    )(*operands.values())
    count = math.gcd(rb, 8)
    passed = [memory_new, mixed_out, normalizer_new, stabilizer_new]
    memory_new, mixed_out, normalizer_new, stabilizer_new = pl.pallas_call(
        functools.partial(results_kernel, count, len(passed)),
        out_shape=[jax.ShapeDtypeStruct(a.shape, a.dtype) for a in passed],
        in_specs=[hbm] * len(passed),
        out_specs=[hbm] * len(passed),
        scratch_shapes=[pltpu.VMEM(a.shape, a.dtype) for a in passed]
        + [dma((count + len(passed) - 1,)), dma((count + len(passed) - 1,))],
    )(*passed)
    return mixed_out, memory_new, normalizer_new, stabilizer_new.T


def solution(mesh):
    kv, tp, both = P("kv"), P("tp"), P("kv", "tp")
    width, back = P(None, "kv"), P("tp", "kv")
    return jax.shard_map(
        functools.partial(on_device, mesh.shape["kv"], mesh.shape["tp"]),
        mesh=mesh,
        in_specs=(width, kv, both, both, back, kv, both, both, both, both, kv, kv, tp, both, both, both,
                  back, kv, both, both, back),
        out_specs=(width, both, both, both),
        check_vma=False,
    )
```

```python
import functools
import math
from types import SimpleNamespace as NS

import jax
import jax.numpy as jnp
from jax import lax
from jax.experimental import pallas as pl
from jax.experimental.pallas import tpu as pltpu
from jax.sharding import PartitionSpec as P

EPSILON = 1e-06
LANES = 128
TILE = 256
PACE = (2, 3, 3, 3)
DIRECT = 1
LAG = 9
JOINED = 0
READY = 0
BLOCKS = 4
MESH = pl.DeviceIdType.MESH
BF = jnp.bfloat16
F32 = jnp.float32


def chunks_of(hidden):
    tiles = -(-hidden // TILE)
    total, passed, cuts = sum(PACE), 0, [0]
    for share in PACE:
        passed += share
        cut = min(hidden, (tiles * passed + total // 2) // total * TILE)
        if cut > cuts[-1]:
            cuts.append(cut)
    return [(low, high - low) for low, high in zip(cuts, cuts[1:])]


def layer_kernel(n_kv, n_tp, unpack, *refs):
    arg, out, mem = unpack(refs)
    nz = n_kv // 2
    me = lax.axis_index("kv")
    z, c = me // 2, lax.rem(me, 2)
    tp = lax.axis_index("tp")
    partner = me + 1 - 2 * c
    rows, width = arg.tokens.shape
    d_model = width * n_kv
    rb = rows // n_kv
    rt = rows // n_tp
    head_size = arg.memory.shape[-1]
    heads = arg.memory.shape[1]

    pieces_of = chunks_of(arg.gate_first.shape[0])
    relayed = max(len(pieces_of) - DIRECT, 0)
    held = NS(**mem.held)
    loads = {}

    def begin(name, cuts=None):
        source, target = getattr(arg, name), mem.held[name]
        for cut in cuts or [None]:
            at = slice(None) if cut is None else pl.ds(*cut)
            sem = mem.load_sem.at[sum(len(made) for made in loads.values())]
            copy = pltpu.make_async_copy(source.at[at], target.at[at], sem)
            copy.start()
            loads.setdefault(name, []).append(copy)

    def loaded(name, i=None):
        for copy in loads[name] if i is None else [loads[name][i]]:
            copy.wait()

    begin("tokens")
    begin("gain_first")
    for cut in pieces_of:
        begin("gate_first", [cut])
        begin("up_first", [cut])
    for name in mem.held:
        if name not in loads:
            begin(name)

    barrier = pltpu.get_barrier_semaphore()
    for d in range(1, n_kv):
        pl.semaphore_signal(barrier, inc=1, device_id={"kv": lax.rem(me + d, n_kv)}, device_id_type=MESH)
    for d in range(1, n_tp):
        pl.semaphore_signal(barrier, inc=1, device_id={"tp": lax.rem(tp + d, n_tp)}, device_id_type=MESH)

    def everyone_here():
        pl.semaphore_wait(barrier, n_kv + n_tp - 2)

    pending = []

    def remote(src, dst, send_sem, recv_sem, where):
        return pltpu.make_async_remote_copy(
            src_ref=src, dst_ref=dst, send_sem=send_sem, recv_sem=recv_sem, device_id=where, device_id_type=MESH)

    def send(*args):
        remote(*args).start()
        pending.append(args)

    def drain():
        for args in pending:
            remote(*args).wait_send()
        pending.clear()

    def arrived(dst, send_sem, recv_sem):
        remote(dst, dst, send_sem, recv_sem, {"kv": partner}).wait_recv()

    def flat(ref):
        a, b, w = ref.shape
        return ref[...].reshape(a * b, w)

    def rows_of(ref):
        return lambda own=None: flat(ref) if own is None else ref[tp]

    def norm_prepare(n, x, gain):
        wide = x.astype(F32)
        mem.scaled[...] = (wide * gain[...]).astype(BF)
        part = jnp.sum(wide * wide, axis=1, keepdims=True)
        n.sq_out[...] = jnp.broadcast_to(part, (rows, LANES)).reshape(n_kv, rb, LANES)

    def norm_send(n):
        for d in range(1, n_kv):
            peer = lax.rem(me + d, n_kv)
            send(n.sq_out.at[peer], n.sq_in.at[d], n.sq_s.at[d], n.sq_r.at[d], {"kv": peer})

    def norm_scale(n):
        total = n.sq_out[me]
        for d in range(1, n_kv):
            arrived(n.sq_in.at[d], n.sq_s.at[d], n.sq_r.at[d])
            total = total + n.sq_in[d]
        return lax.rsqrt(total / d_model + EPSILON)[:, :1]

    def rows_dot(weight):
        return lax.dot_general(
            mem.scaled[...], weight, (((1,), (1,)), ((), ())), preferred_element_type=F32).astype(BF)

    def keep(buf, g, val, place):
        for i in range(n_kv):
            buf[i % 2, i // 2, g, :, place] = val[i * rb:(i + 1) * rb]

    def product(weight, start, size, buf, g):
        step = TILE
        full = size // step

        def tile(off, n, place):
            keep(buf, g, rows_dot(weight[pl.ds(off, n), :]), pl.ds(place, n))

        if full:
            @pl.loop(0, full)
            def _(t):
                tile(pl.multiple_of(start + t * step, 16), step, pl.multiple_of(t * step, step))
        if size > full * step:
            tile(start + full * step, size - full * step, full * step)

    def scatter_pair(s):
        for d in range(nz):
            chip = lax.rem(z + d + 1, nz)
            send(s.a.at[1 - c, chip], s.b.at[chip], s.s1.at[d], s.r1.at[d], {"kv": partner})

    def scatter_chips(s):
        for d in range(nz):
            chip = lax.rem(z + d + 1, nz)
            arrived(s.b.at[chip], s.s1.at[d], s.r1.at[d])
            if d < nz - 1:
                s.c[d] = (s.a[c, chip].astype(F32) + s.b[chip].astype(F32)).astype(BF)
                send(s.c.at[d], s.d.at[d], s.s2.at[d], s.r2.at[d], {"kv": chip * 2 + c})

    def scatter_sum(s):
        total = s.a[c, z].astype(F32) + s.b[z].astype(F32)
        for d in range(nz - 1):
            arrived(s.d.at[d], s.s2.at[d], s.r2.at[d])
            total = total + s.d[d].astype(F32)
        return total

    def gather_start(s):
        for d in range(nz - 1):
            chip = lax.rem(z + d + 1, nz)
            send(s.g.at[me], s.g.at[me], s.gs.at[d], s.gr.at[d], {"kv": chip * 2 + c})
        send(s.g.at[me], s.g.at[me], s.hs.at[nz - 1], s.hr.at[nz - 1], {"kv": partner})

    def gather_forward(s):
        for d in range(nz - 1):
            block = lax.rem(z - d - 1 + nz, nz) * 2 + c
            arrived(s.g.at[block], s.gs.at[d], s.gr.at[d])
            send(s.g.at[block], s.g.at[block], s.hs.at[d], s.hr.at[d], {"kv": partner})

    def gather_wait(s):
        for d in range(nz):
            block = lax.rem(z - d - 1 + nz, nz) * 2 + 1 - c
            arrived(s.g.at[block], s.hs.at[d], s.hr.at[d])

    line = nz == 4
    at_end = (z == 0) | (z == nz - 1)
    mate = z + 1 - 2 * lax.rem(z, 2)
    far_middle = jnp.where(z < 2, 2, 1)
    far_end = jnp.where(z < 2, 3, 0)
    far = (far_middle, far_end)

    def chip_sum(s, chip):
        return s.a[c, chip].astype(F32) + s.b[chip].astype(F32)

    def line_pair(s):
        send(s.a.at[1 - c], s.b, s.s1.at[0], s.r1.at[0], {"kv": partner})

    def line_send_out(s):
        arrived(s.b, s.s1.at[0], s.r1.at[0])

        @pl.when(at_end)
        def _():
            if JOINED:
                for j in (1, 0):
                    s.c[j] = chip_sum(s, far[j]).astype(BF)
                both = pl.ds(0, 2)
                remote(s.c.at[both], s.e, s.s2.at[0], s.re.at[0], {"kv": mate * 2 + c}).start()
            else:
                for j in (1, 0):
                    s.c[j] = chip_sum(s, far[j]).astype(BF)
                    remote(s.c.at[j], s.e.at[j], s.s2.at[j], s.re.at[j], {"kv": mate * 2 + c}).start()

        @pl.when(jnp.logical_not(at_end))
        def _():
            line_send_mate(s)

    def line_send_mate(s):
        s.c[2] = chip_sum(s, mate).astype(BF)
        remote(s.c.at[2], s.d.at[0], s.s2.at[2], s.r2.at[0], {"kv": mate * 2 + c}).start()

    def line_follow(s):
        @pl.when(at_end)
        def _():
            line_send_mate(s)

    def line_pass(s):
        @pl.when(jnp.logical_not(at_end))
        def _():
            for j in (1, 0):
                arrived(s.e.at[j], s.s2.at[j], s.re.at[j])
                s.c[j] = (chip_sum(s, far[j]) + s.e[j].astype(F32)).astype(BF)
                remote(s.c.at[j], s.d.at[1], s.s2.at[j], s.r2.at[1], {"kv": far[j] * 2 + c}).start()

        for j in range(3):
            pending.append((s.c.at[j], s.d.at[0], s.s2.at[j], s.r2.at[0], {"kv": mate * 2 + c}))

    def line_sum(s):
        total = chip_sum(s, z)
        for j in range(2):
            arrived(s.d.at[j], s.s2.at[j], s.r2.at[j])
            total = total + s.d[j].astype(F32)
        return total

    mine = jnp.where(at_end, 2, 1)

    def line_gather_start(s, direct):
        send(s.g.at[me], s.g.at[me], s.gs.at[0], s.gr.at[0], {"kv": mate * 2 + c})
        for j in range(2 if direct else 1):
            send(s.g.at[me], s.g.at[me], s.gs.at[1 + j], s.gr.at[mine], {"kv": far[j] * 2 + c})
        send(s.g.at[me], s.g.at[me], s.hs.at[nz - 1], s.hr.at[nz - 1], {"kv": partner})

    def line_gather_forward(s, direct):
        for j, chip in enumerate((mate, far_middle, far_end)):
            block = chip * 2 + c
            arrived(s.g.at[block], s.gs.at[j], s.gr.at[j])
            if j > 0 and not direct:
                @pl.when(jnp.logical_not(at_end))
                def _():
                    remote(s.g.at[block], s.g.at[block], s.gs.at[j + 1], s.gr.at[j], {"kv": mate * 2 + c}).start()
            send(s.g.at[block], s.g.at[block], s.hs.at[j], s.hr.at[j], {"kv": partner})

    def line_gather_wait(s):
        for j, chip in enumerate((mate, far_middle, far_end, z)):
            arrived(s.g.at[chip * 2 + 1 - c], s.hs.at[j], s.hr.at[j])

    def line_gather_sent(s):
        @pl.when(jnp.logical_not(at_end))
        def _():
            for j in range(1, 3):
                block = far[j - 1] * 2 + c
                remote(s.g.at[block], s.g.at[block], s.gs.at[j + 1], s.gr.at[j], {"kv": mate * 2 + c}).wait_send()

    def sum_tp(n, acc, residual, factor):
        if n_tp == BLOCKS:
            sum_tp_exchange(n, acc, residual(), factor)
        else:
            drain()
            sum_tp_scatter(n, acc, residual(own_tp), factor)

    def sum_tp_exchange(n, acc, residual, factor):
        half = width // 2
        sub = rows // BLOCKS
        one, two = tp + 1 - 2 * lax.rem(tp, 2), lax.rem(tp + 2, 4)
        order = [(k, r) for r in range(BLOCKS) for k in range(2)]

        def part(val, k, r):
            return val[r * sub:(r + 1) * sub, k * half:(k + 1) * half]

        def swap(step, k, r):
            i = (step * 2 + k) * BLOCKS + r
            return n.p.at[i], n.q.at[i], n.ps.at[i], n.pr.at[i], {"tp": one if k == step else two}

        for k, r in order:
            n.p[k * BLOCKS + r] = part(acc, k, r).astype(BF)
            send(*swap(0, k, r))
        started = pending[-len(order):]
        del pending[-len(order):]
        drain()
        pending.extend(started)
        for k, r in order:
            i = k * BLOCKS + r
            arrived(n.q.at[i], n.ps.at[i], n.pr.at[i])
            n.p[2 * BLOCKS + i] = (n.p[i].astype(F32) + n.q[i].astype(F32)).astype(BF)
            send(*swap(1, k, r))
        for k, r in order:
            i = (2 + k) * BLOCKS + r
            arrived(n.q.at[i], n.ps.at[i], n.pr.at[i])
            total = n.p[i].astype(F32) + n.q[i].astype(F32)
            val = (part(residual, k, r).astype(F32) + factor * total).astype(BF)
            n.o[r, :, k * half:(k + 1) * half] = val

    def sum_tp_scatter(n, acc, residual, factor):
        mem.acc[...] = acc
        for j in range(n_tp):
            n.p[j] = acc[j * rt:(j + 1) * rt].astype(BF)
        for d in range(1, n_tp):
            peer = lax.rem(tp + d, n_tp)
            send(n.p.at[peer], n.q.at[d], n.ps.at[d], n.pr.at[d], {"tp": peer})
        total = mem.acc[pl.ds(pl.multiple_of(tp * rt, rt), rt)]
        for d in range(1, n_tp):
            arrived(n.q.at[d], n.ps.at[d], n.pr.at[d])
            total = total + n.q[d].astype(F32)
        n.o[tp] = (residual.astype(F32) + factor * total).astype(BF)
        for d in range(1, n_tp):
            peer = lax.rem(tp + d, n_tp)
            send(n.o.at[tp], n.o.at[tp], n.os.at[d], n.ur.at[d], {"tp": peer})
        for d in range(1, n_tp):
            source = lax.rem(tp - d + n_tp, n_tp)
            arrived(n.o.at[source], n.os.at[d], n.ur.at[d])

    def send_out(pieces, i):
        if not line:
            scatter_chips(pieces[i][1])
            return
        line_send_out(pieces[i][1])
        if i >= LAG:
            line_follow(pieces[i - LAG][1])

    def half_step(label, n, x, residual, ready=None):
        gate, up, down = (mem.held[name + label] for name in ("gate_", "up_", "down_"))
        norm_prepare(n, x, mem.held["gain_" + label])
        if ready is None:
            norm_send(n)
        pieces = list(zip(pieces_of, n.parts))
        by_piece = len(loads["gate_" + label]) > 1
        pair = line_pair if line else scatter_pair
        held_back = min(READY, len(pieces) - 1)
        for i, ((start, size), s) in enumerate(pieces):
            if by_piece or i == 0:
                loaded("gate_" + label, i)
            product(gate, start, size, s.a, 0)
            if by_piece or i == 0:
                loaded("up_" + label, i)
            product(up, start, size, s.a, 1)
            if ready is not None and i < held_back:
                continue
            if ready is not None and i == held_back:
                ready()
                norm_send(n)
                for _, earlier in pieces[:i]:
                    pair(earlier)
            pair(s)
            for j in range(0 if i == held_back and ready is not None else max(i - 1, 0), i):
                send_out(pieces, j)
        send_out(pieces, len(pieces) - 1)
        scale = norm_scale(n)
        drain()
        if line:
            for _, s in pieces[max(len(pieces) - LAG, 0):]:
                line_follow(s)
            for _, s in pieces:
                line_pass(s)
        for i, (_, s) in enumerate(pieces):
            total = (line_sum if line else scatter_sum)(s)
            gate_values, up_values = scale * total[0], scale * total[1]
            s.g[me] = (gate_values / (1.0 + jnp.exp(-gate_values)) * up_values).astype(BF)
            if line:
                line_gather_start(s, i >= relayed)
            else:
                gather_start(s)
        for i, (_, s) in enumerate(pieces):
            if line:
                line_gather_forward(s, i >= relayed)
            else:
                gather_forward(s)
        loaded("down_" + label)
        acc = jnp.zeros((rows, width), F32)
        for (start, size), s in pieces:
            (line_gather_wait if line else gather_wait)(s)
            acc = acc + jnp.dot(flat(s.g), down[start:start + size, :], preferred_element_type=F32)
        sum_tp(n, acc, residual, 0.5)
        if line:
            for _, s in pieces[:relayed]:
                line_gather_sent(s)

    own_tp = pl.ds(pl.multiple_of(tp * rt, rt), rt)
    loaded("tokens")
    loaded("gain_first")
    half_step("first", mem.first, held.tokens[...], lambda own=slice(None): held.tokens[own], everyone_here)
    for name in ("gain_mix", "w_ingate", "w_forget", "normalizer", "stabilizer", "gain_second"):
        loaded(name)

    n = mem.mix
    norm_prepare(n, flat(mem.first.o), held.gain_mix)
    norm_send(n)
    dm = held.w_query.shape[1]
    n_heads = held.w_ingate.shape[0]
    one, two = n.parts

    def wide_product(weight, s, at):
        val = jnp.dot(mem.scaled[...], weight[...], preferred_element_type=F32).astype(BF)
        keep(s.a, 0, val, slice(at, at + dm))

    loaded("w_query")
    wide_product(held.w_query, one, 0)
    loaded("w_key")
    wide_product(held.w_key, one, dm)
    gates = rows_dot(jnp.concatenate([held.w_ingate[...], held.w_forget[...]], axis=0))
    gates = jnp.concatenate([gates, jnp.zeros((rows, LANES - 2 * n_heads), BF)], axis=1)
    keep(one.a, 0, gates, slice(2 * dm, 2 * dm + LANES))
    scatter_pair(one)
    loaded("w_value")
    wide_product(held.w_value, two, 0)
    loaded("w_outgate")
    wide_product(held.w_outgate, two, dm)
    scatter_pair(two)
    scatter_chips(one)
    scatter_chips(two)
    scale = norm_scale(n)
    total = scale * scatter_sum(one)[0]
    total_two = scale * scatter_sum(two)[0]

    gates = total[:, 2 * dm:]
    lane = lax.broadcasted_iota(jnp.int32, (rb, LANES), 1)
    diagonal = lax.broadcasted_iota(jnp.int32, (rb, rb), 0) == lax.broadcasted_iota(jnp.int32, (rb, rb), 1)
    loaded("memory")
    state = held.memory
    parts = []
    for h in range(heads):
        low, high = h * head_size, (h + 1) * head_size
        q, k, v, gate_out = (
            val.astype(BF).astype(F32)
            for val in (total[:, low:high], total[:, dm + low:dm + high],
                        total_two[:, low:high], total_two[:, dm + low:dm + high]))
        k = k * head_size ** (-0.5)
        ingate = jnp.sum(jnp.where(lane == tp * heads + h, gates, 0.0), axis=1, keepdims=True)
        forget = jnp.sum(jnp.where(lane == n_heads + tp * heads + h, gates, 0.0), axis=1, keepdims=True)
        forget = forget + arg.forget_bias[h]
        log_forget = jnp.minimum(forget, 0.0) - jnp.log1p(jnp.exp(-jnp.abs(forget)))
        stabilizer = jnp.sum(jnp.where(diagonal, held.stabilizer[h:h + 1, :], 0.0), axis=1, keepdims=True)
        kept = log_forget + stabilizer
        ceiling = jnp.maximum(kept, ingate)
        fresh = jnp.exp(ingate - ceiling)
        carried = jnp.exp(kept - ceiling)
        out.stabilizer_new[h:h + 1, :] = jnp.sum(jnp.where(diagonal, ceiling, 0.0), axis=0, keepdims=True)
        norm = held.normalizer[:, h, :]
        out.normalizer_new[:, h, :] = carried * norm + fresh * k
        own = jnp.sum(q * k, axis=1, keepdims=True) * fresh
        den = own + carried * jnp.sum(norm * q, axis=1, keepdims=True)
        den = jnp.maximum(jnp.abs(den), jnp.exp(-ceiling))
        mem.row_q[h] = q
        mem.row_k[h] = fresh * k
        mem.row_c[h] = jnp.broadcast_to(carried, (rb, head_size))
        pad = jnp.zeros((LANES - rb, head_size), F32)
        mem.col_v[h] = jnp.concatenate([v, pad], axis=0).T
        parts.append((own, v, carried, den, gate_out))

    lane2 = lax.broadcasted_iota(jnp.int32, (head_size, LANES), 1)
    row = lax.broadcasted_iota(jnp.int32, (rb, head_size), 0)
    queries = [mem.row_q[h].astype(BF) for h in range(heads)]
    together = math.gcd(rb, 4)

    def recall_step(step, found):
        for at in range(together):
            b = step * together + at
            found = tuple(
                jnp.where(row == b, lax.dot_general(
                    queries[h], state[b, h].astype(BF), (((1,), (1,)), ((), ())), preferred_element_type=F32), found[h])
                for h in range(heads))
        return found

    nothing = jnp.zeros((rb, head_size), F32)
    recalls = lax.fori_loop(0, rb // together, recall_step, (nothing,) * heads)

    for h in range(heads):
        own, v, carried, den, gate_out = parts[h]
        recall = recalls[h]
        readout = (own * v + carried * recall) / den
        n.parts[0].g[me, :, h * head_size:(h + 1) * head_size] = (
            readout / (1.0 + jnp.exp(-gate_out))).astype(BF)
    gather_start(one)

    @pl.loop(0, rb)
    def _(b):
        for h in range(heads):
            v_col = jnp.sum(jnp.where(lane2 == b, mem.col_v[h], 0.0), axis=1, keepdims=True)
            state[b, h] = (mem.row_c[h, pl.ds(b, 1), :] * state[b, h]
                           + v_col * mem.row_k[h, pl.ds(b, 1), :])

    store = pltpu.make_async_copy(state, out.memory_new, mem.load_sem.at[sum(len(made) for made in loads.values())])
    store.start()
    gather_forward(one)
    loaded("w_project")
    gather_wait(one)
    sum_tp(n, jnp.dot(flat(one.g), held.w_project[...], preferred_element_type=F32), rows_of(mem.first.o), 1.0)

    half_step("second", mem.second, flat(n.o), rows_of(n.o))
    out.mixed_out[...] = flat(mem.second.o)
    store.wait()
    drain()


def results_kernel(count, n, *refs):
    sources, targets, held, (in_sem, out_sem) = refs[:n], refs[n:2 * n], refs[2 * n:3 * n], refs[3 * n:]
    pieces = []
    for source, target, ref in zip(sources, targets, held):
        cuts = count if source is sources[0] else 1
        size = ref.shape[0] // cuts
        for i in range(cuts):
            at = pl.ds(i * size, size)
            sems = len(pieces)
            pieces.append((
                pltpu.make_async_copy(source.at[at], ref.at[at], in_sem.at[sems]),
                pltpu.make_async_copy(ref.at[at], target.at[at], out_sem.at[sems])))
    for into, _ in pieces:
        into.start()
    for into, out in pieces:
        into.wait()
        out.start()
    for _, out in pieces:
        out.wait()


def on_device(
    n_kv, n_tp, tokens, gain_first, gate_first, up_first, down_first, gain_mix, w_query, w_key, w_value,
    w_outgate, w_ingate, w_forget, forget_bias, memory, normalizer, stabilizer, w_project, gain_second,
    gate_second, up_second, down_second,
):
    rows, width = tokens.shape
    hidden = gate_first.shape[1]
    dm = w_query.shape[1]
    nz, rb, rt = n_kv // 2, rows // n_kv, rows // n_tp
    heads, head_size = memory.shape[1], memory.shape[3]
    dma = pltpu.SemaphoreType.DMA

    in_smem = dict(forget_bias=forget_bias)
    streamed = dict(
        tokens=tokens, gain_first=gain_first.reshape(1, -1), gate_first=gate_first.T, up_first=up_first.T,
        down_first=down_first, gain_mix=gain_mix.reshape(1, -1), w_ingate=w_ingate.T, w_forget=w_forget.T,
        w_query=w_query, w_key=w_key, w_value=w_value, w_outgate=w_outgate, normalizer=normalizer,
        stabilizer=stabilizer.T, memory=memory, w_project=w_project, gain_second=gain_second.reshape(1, -1),
        gate_second=gate_second.T, up_second=up_second.T, down_second=down_second)
    operands = {**in_smem, **streamed}
    results = dict(
        mixed_out=jax.ShapeDtypeStruct(tokens.shape, BF),
        memory_new=jax.ShapeDtypeStruct(memory.shape, F32),
        normalizer_new=jax.ShapeDtypeStruct(normalizer.shape, F32),
        stabilizer_new=jax.ShapeDtypeStruct(stabilizer.shape[::-1], F32))

    line = nz == 4

    def signals(joined, gathered):
        counts = dict(s1=nz, r1=nz, s2=nz, r2=nz)
        if gathered:
            counts.update(gs=nz, gr=nz, hs=nz, hr=nz)
        if joined and line:
            counts.update(s1=1, r1=1, s2=3, r2=2, re=2, gr=3)
        return {name: dma((count,)) for name, count in counts.items()}

    def exchange(g, cols, gathered, sems):
        bufs = dict(
            a=pltpu.VMEM((2, nz, g, rb, cols), BF), b=pltpu.VMEM((nz, g, rb, cols), BF),
            c=pltpu.VMEM((nz, g, rb, cols), BF), d=pltpu.VMEM((nz, g, rb, cols), BF), **sems)
        if g == 2 and line:
            bufs.update(e=pltpu.VMEM((2, g, rb, cols), BF))
        if gathered:
            bufs.update(g=pltpu.VMEM((n_kv, rb, gathered), BF))
        return bufs

    traded = n_tp == BLOCKS
    swap = (4 * BLOCKS, rows // BLOCKS, width // 2) if traded else (n_tp, rt, width)
    squares = dict(sq_s=dma((n_kv,)), sq_r=dma((n_kv,)))

    def sums():
        made = dict(ps=dma(swap[:1]), pr=dma(swap[:1]))
        return made if traded else dict(os=dma((n_tp,)), ur=dma((n_tp,)), **made)

    def phase(parts, tp_sems):
        return dict(
            parts=parts,
            sq_out=pltpu.VMEM((n_kv, rb, LANES), F32), sq_in=pltpu.VMEM((n_kv, rb, LANES), F32),
            p=pltpu.VMEM(swap, BF), q=pltpu.VMEM(swap, BF), o=pltpu.VMEM((n_tp, rt, width), BF),
            **squares, **tp_sems)

    cuts = chunks_of(hidden)
    half_sems, half_sums = [signals(True, True) for _ in cuts], sums()

    def half():
        return phase([exchange(2, size, size, sems) for (_, size), sems in zip(cuts, half_sems)], half_sums)

    tree = dict(
        held={name: pltpu.VMEM(a.shape, a.dtype) for name, a in streamed.items()},
        load_sem=dma((len(streamed) + 2 * len(chunks_of(hidden)),)),
        scaled=pltpu.VMEM((rows, width), BF),
        acc=pltpu.VMEM((rows, width), F32),
        first=half(),
        mix=phase([exchange(1, 2 * dm + LANES, dm, signals(False, True)),
                   exchange(1, 2 * dm, 0, signals(False, False))], sums()),
        second=half(),
        row_q=pltpu.VMEM((heads, rb, head_size), F32),
        row_k=pltpu.VMEM((heads, rb, head_size), F32),
        row_c=pltpu.VMEM((heads, rb, head_size), F32),
        col_v=pltpu.VMEM((heads, head_size, LANES), F32))

    shapes = []

    def number(node):
        if isinstance(node, dict):
            return {key: number(value) for key, value in node.items()}
        if isinstance(node, list):
            return [number(value) for value in node]
        for at, shape in enumerate(shapes):
            if shape is node:
                return at
        shapes.append(node)
        return len(shapes) - 1

    numbered = number(tree)

    def unpack(refs):
        n_in, n_out = len(operands), len(results)
        scratch = refs[n_in + n_out:]

        def fill(node):
            if isinstance(node, dict):
                return NS(**{key: fill(value) for key, value in node.items()})
            if isinstance(node, list):
                return [fill(value) for value in node]
            return scratch[node]

        mem = fill(numbered)
        mem.held = {name: scratch[i] for name, i in numbered["held"].items()}
        return NS(**dict(zip(operands, refs))), NS(**dict(zip(results, refs[n_in:]))), mem

    vm = pl.BlockSpec(memory_space=pltpu.VMEM)
    hbm = pl.BlockSpec(memory_space=pl.ANY)
    mixed_out, memory_new, normalizer_new, stabilizer_new = pl.pallas_call(
        functools.partial(layer_kernel, n_kv, n_tp, unpack),
        out_shape=list(results.values()),
        in_specs=[pl.BlockSpec(memory_space=pltpu.SMEM)] + [hbm] * len(streamed),
        out_specs=[vm, hbm, vm, vm],
        scratch_shapes=shapes,
        compiler_params=pltpu.CompilerParams(
            collective_id=0, has_side_effects=True, vmem_limit_bytes=60 * 2**20),
    )(*operands.values())
    count = math.gcd(rb, 8)
    passed = [memory_new, mixed_out, normalizer_new, stabilizer_new]
    memory_new, mixed_out, normalizer_new, stabilizer_new = pl.pallas_call(
        functools.partial(results_kernel, count, len(passed)),
        out_shape=[jax.ShapeDtypeStruct(a.shape, a.dtype) for a in passed],
        in_specs=[hbm] * len(passed),
        out_specs=[hbm] * len(passed),
        scratch_shapes=[pltpu.VMEM(a.shape, a.dtype) for a in passed]
        + [dma((count + len(passed) - 1,)), dma((count + len(passed) - 1,))],
    )(*passed)
    return mixed_out, memory_new, normalizer_new, stabilizer_new.T


def solution(mesh):
    kv, tp, both = P("kv"), P("tp"), P("kv", "tp")
    width, back = P(None, "kv"), P("tp", "kv")
    return jax.shard_map(
        functools.partial(on_device, mesh.shape["kv"], mesh.shape["tp"]),
        mesh=mesh,
        in_specs=(width, kv, both, both, back, kv, both, both, both, both, kv, kv, tp, both, both, both,
                  back, kv, both, both, back),
        out_specs=(width, both, both, both),
        check_vma=False,
    )
```
